512 devices in a mesh: ep: 128 (over z, y, core), tp: 4 (over x).
Axes of the slice: x: 4, y: 8, z: 8, core: 2. Of those that a mesh axis runs over, the one named last changes fastest.
Arguments:
- tokens: bfloat16 [16384, 2048], P('ep'), may hold values from -6 to 6
- norm_gain: float32 [2048], replicated, may hold values from 0.1 to 1.9
- routes: int32 [16384, 2], P('ep'), may hold values from 0 to 31, as said below
- route_scores: float32 [16384, 2], P('ep'), may hold values from -6 to 6
- expert_gate: bfloat16 [128, 2048, 1024], P('ep', None, 'tp'), may hold values from -0.125 to 0.125
- expert_up: bfloat16 [128, 2048, 1024], P('ep', None, 'tp'), may hold values from -0.125 to 0.125
- expert_down: bfloat16 [128, 1024, 2048], P('ep', None, 'tp'), may hold values from -0.09375 to 0.09375
- branch_in: bfloat16 [2048, 512], P('ep', 'tp'), may hold values from -0.125 to 0.125
- branch_out: bfloat16 [512, 2048], P('tp', 'ep'), may hold values from -0.25 to 0.25
- branch_gate: float32 [2048], replicated, may hold values from -0.125 to 0.125
Outputs:
- mixed: bfloat16 [16384, 2048], P('ep', 'tp')
The draws below stay inside these ranges and needn't reach their ends.
Inputs may be any that keep to these rules, and one draw needn't show every extreme that they name: `routes`: each row names 2 different experts. In each aligned block of 128 rows (the rows of one index of ep) no expert is named more than 10 times, and one expert, the same in every block, is named exactly 10 times in every block.
All inputs are finite; a program needn't handle non-finite values.
Results may differ from the reference program's by a relative error of at most 0.0066.
Values may be sent and summed in bfloat16 or wider, within the bound.
A program may use at most 64 MiB of HBM per device.

```python
from functools import partial
import jax
import jax.numpy as jnp
from jax import lax

D = 2048
FF = 4096
DB = 512
TOP = 2
TOK_DEV = 128
GROUP = 4
EXPERTS = 32
FF_PART = 1024
CAP = 10
TOKENS = 16384
N_EP = 128


def route_block(block_key, popular, full_expert):
    pool_size = EXPERTS * CAP
    pool = jnp.arange(pool_size, dtype=jnp.int32) // CAP
    noise_key, order_key = jax.random.split(block_key)
    noise = jax.random.randint(noise_key, (pool_size,), 0, 64, dtype=jnp.int32)
    serial = jnp.arange(pool_size, dtype=jnp.int32)
    score = (noise + popular[pool]) * pool_size + serial
    score = jnp.where(pool == full_expert, 200 * pool_size + serial, score)
    ranked = jnp.argsort(-score, stable=True)
    kept = jnp.sort(ranked[:TOP * TOK_DEV])
    chosen = pool[kept]
    pairs = jnp.stack([chosen[:TOK_DEV], chosen[TOK_DEV:]], axis=1)
    shuffle = jax.random.permutation(order_key, TOK_DEV)
    return pairs[shuffle]


def draw_routes(key, part):
    base = jax.random.fold_in(key, 7)
    full_key, popular_key, block_key = jax.random.split(base, 3)
    full_expert = jax.random.randint(full_key, (), 0, EXPERTS, dtype=jnp.int32)
    popular = jax.random.randint(popular_key, (EXPERTS,), 0, 48, dtype=jnp.int32)
    block_keys = jax.random.split(block_key, TOKENS // TOK_DEV)
    blocks = jax.vmap(partial(route_block, popular=popular, full_expert=full_expert))(block_keys)
    return blocks.reshape(TOKENS, TOP).astype(jnp.int32)


def steps_of(rng, shape, pieces, low, largest):
    def one(dim, blocks):
        draws = jax.random.uniform(jax.random.fold_in(jax.random.fold_in(rng, 6), dim), (blocks,), jnp.float32, low / len(pieces), largest / len(pieces))
        return jnp.repeat(jnp.exp(draws), shape[dim] // blocks).reshape((-1,) + (1,) * (len(shape) - dim - 1))

    level = one(*pieces[0])
    for cut in pieces[1:]:
        level = level * one(*cut)
    return level


def scatter_about(key, extent, spread, reach, shards=(), kind=jnp.bfloat16):
    entries = spread * jax.random.normal(key, extent, jnp.float32)
    if shards:
        entries = entries * steps_of(key, extent, shards, -0.22, 0.18)
    return jnp.clip(entries, -reach, reach).astype(kind)


def setup_inputs(seed: int = 0) -> dict:
    streams_of = jax.random.split(jax.random.key(seed), 11)
    tokens = scatter_about(streams_of[0], (TOKENS, D), 1.0, 6.0, ((0, 128),))
    norm_gain = jnp.clip(1.0 + 0.18 * jax.random.normal(streams_of[1], (D,), jnp.float32), 0.1, 1.9)
    routes = draw_routes(jax.random.fold_in(streams_of[10], 71), 0)
    route_scores = scatter_about(streams_of[3], (TOKENS, TOP), 1.5, 6.0, ((0, 128),), jnp.float32)
    expert_gate = scatter_about(streams_of[4], (EXPERTS * GROUP, D, FF_PART), D ** -0.5, 0.125, ((0, 128), (2, 4)))
    expert_up = scatter_about(streams_of[5], (EXPERTS * GROUP, D, FF_PART), D ** -0.5, 0.125, ((0, 128), (2, 4)))
    expert_down = scatter_about(streams_of[6], (EXPERTS * GROUP, FF_PART, D), FF ** -0.5, 0.09375, ((0, 128), (2, 4)))
    branch_in = scatter_about(streams_of[7], (D, DB), D ** -0.5, 0.125, ((0, 128), (1, 4)))
    branch_out = scatter_about(streams_of[8], (DB, D), DB ** -0.5, 0.25, ((0, 4), (1, 128)))
    branch_gate = scatter_about(streams_of[9], (D,), D ** -0.5, 0.125, (), jnp.float32)
    return dict(tokens=tokens, norm_gain=norm_gain, routes=routes, route_scores=route_scores, expert_gate=expert_gate, expert_up=expert_up, expert_down=expert_down, branch_in=branch_in, branch_out=branch_out, branch_gate=branch_gate)


NORM_EPSILON = 1e-06

def reference(tokens, norm_gain, routes, route_scores, expert_gate, expert_up, expert_down, branch_in, branch_out, branch_gate):
    tokens_float = tokens.astype(jnp.float32)
    scaled = lax.rsqrt(lax.optimization_barrier(jnp.mean(tokens_float * tokens_float, axis=-1, keepdims=True)) + NORM_EPSILON)
    normed = (tokens_float * scaled * norm_gain).astype(jnp.bfloat16)
    difference = route_scores[:, 0] - route_scores[:, 1]
    route_weight = jnp.stack([jax.nn.sigmoid(difference), jax.nn.sigmoid(-difference)], axis=1)
    flat_weight = route_weight.reshape(-1)
    blocks = routes.reshape(N_EP, TOK_DEV * TOP)
    choose = (blocks[:, :, None] == jnp.arange(EXPERTS, dtype=jnp.int32)[None, None, :]).astype(jnp.int32)
    earlier = jnp.cumsum(choose, axis=1, dtype=jnp.int32) - choose
    slot_index = lax.optimization_barrier(jnp.sum(earlier * choose, axis=2, dtype=jnp.int32))
    source_base = jnp.arange(N_EP, dtype=jnp.int32)[:, None] * CAP
    slot_place = (source_base + slot_index).reshape(-1).astype(jnp.int32)
    flat_ids = routes.reshape(-1).astype(jnp.int32)
    owner_token = jnp.arange(TOKENS * TOP, dtype=jnp.int32) // TOP

    def one_expert(running, expert):
        selected = flat_ids == expert
        target = jnp.where(selected, slot_place, N_EP * CAP).astype(jnp.int32)
        row_index = jnp.zeros((N_EP * CAP,), jnp.int32).at[target].set(owner_token, mode='drop')
        row_scale = jnp.zeros((N_EP * CAP,), jnp.float32).at[target].set(flat_weight, mode='drop')
        picked = normed[row_index]
        start = (expert * GROUP).astype(jnp.int32)
        gate_block = lax.dynamic_slice_in_dim(expert_gate, start, GROUP, 0)
        gate_block = jnp.transpose(gate_block, (1, 0, 2)).reshape(D, FF)
        up_block = lax.dynamic_slice_in_dim(expert_up, start, GROUP, 0)
        up_block = jnp.transpose(up_block, (1, 0, 2)).reshape(D, FF)
        down_block = lax.dynamic_slice_in_dim(expert_down, start, GROUP, 0).reshape(FF, D)
        gate_pre = jnp.dot(picked, gate_block, preferred_element_type=jnp.float32)
        up_pre = jnp.dot(picked, up_block, preferred_element_type=jnp.float32)
        hidden = (jax.nn.silu(gate_pre) * up_pre).astype(jnp.bfloat16)
        result = jnp.dot(hidden, down_block, preferred_element_type=jnp.float32)
        running = running.at[row_index].add(row_scale[:, None] * result)
        return (running, None)
    routed, _ = lax.scan(one_expert, jnp.zeros((TOKENS, D), jnp.float32), jnp.arange(EXPERTS, dtype=jnp.int32))
    branch_hidden = jax.nn.silu(jnp.dot(normed, branch_in, preferred_element_type=jnp.float32)).astype(jnp.bfloat16)
    branch_value = jnp.dot(branch_hidden, branch_out, preferred_element_type=jnp.float32)
    branch_weight = jax.nn.sigmoid(lax.optimization_barrier(jnp.sum(normed.astype(jnp.float32) * branch_gate, axis=-1)))
    return (routed + branch_weight[:, None] * branch_value).astype(jnp.bfloat16)
```

```python
import functools

import jax
import jax.numpy as jnp
from jax import lax
from jax.experimental import pallas as pl
from jax.experimental.pallas import tpu as pltpu
from jax.sharding import PartitionSpec as P

NORM_EPSILON = 1e-06
GROUP = 4
CORES = 2
MESH_ID = pl.DeviceIdType.MESH


def round_up(n, m):
    return (n + m - 1) // m * m


def sigmoid(v):
    return 1.0 / (1.0 + jnp.exp(-v))


def floor_div(v, n):
    return jnp.floor((v + 0.5) * (1.0 / n))


def layer_kernel(
    zs_n,
    ys_n,
    xs_n,
    cap,
    tokens,
    gain,
    routes,
    routes_t,
    scores,
    bgate,
    bweights,
    w_gate,
    w_up,
    w_down,
    out,
    normed,
    zsend,
    zrecv,
    ysend,
    tok,
    w_gu,
    w_dn,
    hid,
    acc,
    psend,
    precv,
    half,
    qsend,
    qrecv,
    fsend,
    yback,
    zback,
    zgot,
    bw,
    bterm,
    bgot,
    local_sem,
    zd_s,
    zd_r,
    yd_s,
    yd_r,
    tx_s,
    tx_r,
    tc_s,
    tc_r,
    hx_s,
    hx_r,
    pc_s,
    pc_r,
    qy_s,
    qy_r,
    fy_s,
    fy_r,
    zb_s,
    zb_r,
    by_s,
    by_r,
    bz_s,
    bz_r,
    bc_s,
    bc_r,
    bx_s,
    bx_r,
):
    f32, bf16 = jnp.float32, jnp.bfloat16
    ep = lax.axis_index("ep")
    x = lax.axis_index("tp")
    c = lax.rem(ep, CORES)
    y = lax.rem(ep // CORES, ys_n)
    z = ep // (CORES * ys_n)
    pairs = ys_n // 2
    pair = y // 2
    h = lax.rem(y, 2)
    rows_tok, width = tokens.shape
    dx = width // xs_n
    fx = w_gate.shape[2]
    experts = zs_n * pairs
    zrow = zsend.shape[1]
    erow = ysend.shape[1]

    def at(z_, y_, c_, x_):
        return ((z_ * ys_n + y_) * CORES + c_, x_)

    def zpeer(r):
        return lax.rem(z + r, zs_n)

    def ypeer(r):
        return lax.rem(y + r, ys_n)

    def xpeer(r):
        return lax.rem(x + r, xs_n)

    def remote(src, dst, s, r, dev):
        return pltpu.make_async_remote_copy(
            src_ref=src, dst_ref=dst, send_sem=s, recv_sem=r, device_id=dev, device_id_type=MESH_ID
        )

    barrier = pltpu.get_barrier_semaphore()
    peers = [at(zpeer(r), y, c, x) for r in range(1, zs_n)]
    peers += [at(z, ypeer(r), c, x) for r in range(1, ys_n)]
    peers += [at(z, y, c, xpeer(r)) for r in range(1, xs_n)]
    peers += [at(z, y, 1 - c, x)]
    for dev in peers:
        pl.semaphore_signal(barrier, inc=1, device_id=dev, device_id_type=MESH_ID)

    weights = [
        pltpu.make_async_copy(w_gate.at[0], w_gu.at[:, pl.ds(0, fx)], local_sem.at[0]),
        pltpu.make_async_copy(w_up.at[0], w_gu.at[:, pl.ds(fx, fx)], local_sem.at[1]),
        pltpu.make_async_copy(w_down.at[0], w_dn, local_sem.at[2]),
    ]
    for copy in weights:
        copy.start()

    tf = tokens[...].astype(f32)
    scaled = lax.rsqrt(jnp.sum(tf * tf, axis=-1, keepdims=True) * (1.0 / width) + NORM_EPSILON)
    nf = (tf * scaled * gain[...]).astype(bf16)
    normed[...] = nf
    bsum = jnp.sum(nf.astype(f32) * bgate[...], axis=-1, keepdims=True)
    branch_weight = sigmoid(bsum)

    def positions(r0, r1, axis):
        shape = (experts, rows_tok) if axis == 0 else (rows_tok, experts)
        ids = lax.broadcasted_iota(jnp.int32, shape, axis)
        c0 = jnp.where(ids == r0, 1.0, 0.0)
        c1 = jnp.where(ids == r1, 1.0, 0.0)
        sq = (rows_tok, rows_tok)
        a = lax.broadcasted_iota(jnp.int32, sq, 0)
        b = lax.broadcasted_iota(jnp.int32, sq, 1)
        both = (c0 + c1).astype(bf16)
        if axis == 0:
            earlier = jnp.where(a < b, 1.0, 0.0).astype(bf16)
            rank = jnp.dot(both, earlier, preferred_element_type=f32)
        else:
            earlier = jnp.where(b < a, 1.0, 0.0).astype(bf16)
            rank = jnp.dot(earlier, both, preferred_element_type=f32)

        def place(ch, r):
            e = r.astype(f32)
            zz = floor_div(e, pairs)
            base = zz * zrow + (e - zz * pairs) * cap
            return jnp.sum(ch * rank, axis=axis, keepdims=True) + base

        return place(c0, r0), place(c1, r1)

    p0, p1 = positions(routes_t[0:1, :], routes_t[1:2, :], 0)
    slots = zs_n * zrow
    srow = lax.broadcasted_iota(jnp.int32, (slots, rows_tok), 0).astype(f32)
    pick = jnp.where((srow == p0) | (srow == p1), 1.0, 0.0).astype(bf16)
    own_cols = pl.ds(pl.multiple_of(x * dx, dx), dx)
    packed = jnp.dot(pick, normed[:, own_cols], preferred_element_type=f32).astype(bf16)
    zsend[...] = packed.reshape(zs_n, zrow, dx)

    pl.semaphore_wait(barrier, len(peers))

    zd = []
    for r in range(1, zs_n):
        zt = zpeer(r)
        copy = remote(
            zsend.at[zt], zrecv.at[z], zd_s.at[r], zd_r.at[r], at(zt, y, c, x)
        )
        copy.start()
        zd.append(copy)
    by = []
    for r in range(1, ys_n):
        copy = remote(
            bweights, bw.at[:, z, y, c], by_s.at[r], by_r.at[r], at(z, ypeer(r), c, x)
        )
        copy.start()
        by.append(copy)
    bw[:, z, y, c] = bweights[...]
    zrecv[z] = zsend[z]

    def row_target(q):
        pp = floor_div(q, erow)
        rem = q - pp * erow
        zz = floor_div(rem, cap)
        return jnp.where(zz < zs_n, zz * zrow + pp * cap + (rem - zz * cap), -1.0)

    qcol = lax.broadcasted_iota(jnp.int32, (pairs * erow, slots), 0).astype(f32)
    qlane = lax.broadcasted_iota(jnp.int32, (pairs * erow, slots), 1).astype(f32)
    repack = jnp.where(row_target(qcol) == qlane, 1.0, 0.0).astype(bf16)

    for copy in zd:
        copy.wait_recv()
    arrived = zrecv[...].reshape(slots, dx)
    moved = jnp.dot(repack, arrived, preferred_element_type=f32).astype(bf16)
    ysend[...] = moved.reshape(pairs, erow, dx)

    yd = []
    for r in range(1, ys_n):
        yt = ypeer(r)
        pt = yt // 2
        d = lax.rem(y + ys_n - 2 * pt, ys_n)
        k = jnp.where(d <= pairs, jnp.maximum(2 * d - 1, 0), 2 * (ys_n - d))
        copy = remote(
            ysend.at[pt],
            tok.at[k, c, :, own_cols],
            yd_s.at[r],
            yd_r.at[k],
            at(z, yt, c, x),
        )
        copy.start()
        yd.append(copy)
    tok[h, c, :, own_cols] = ysend[pair]

    for copy in by:
        copy.wait_recv()
    bz = []
    for r in range(1, zs_n):
        zt = zpeer(r)
        part = bw.at[:, z, :, c]
        copy = remote(part, part, bz_s.at[r], bz_r.at[r], at(zt, y, c, x))
        copy.start()
        bz.append(copy)

    east, west = at(z, y, c, xpeer(1)), at(z, y, c, xpeer(xs_n - 1))
    partner = at(z, y, 1 - c, x)
    started = []

    def tok_part(k, xx):
        return tok.at[k, c, :, pl.ds(pl.multiple_of(xx * dx, dx), dx)]

    def hid_part(k, xx):
        return hid.at[k, :, :, pl.ds(pl.multiple_of(xx * fx, fx), fx)]

    def spread(part, sems, rsems, k):
        for way, dev in ((0, east), (1, west)):
            copy = remote(part(k, x), part(k, x), sems.at[way, k], rsems.at[way, k], dev)
            copy.start()
            started.append(copy)

    def arrive(part, rsems, sems, way, k):
        ref = part(k, x)
        remote(ref, ref, sems.at[way, k], rsems.at[way, k], east).wait_recv()

    def relay(part, sems, rsems, k):
        way = k % 2
        arrive(part, rsems, sems, way, k)
        ref = part(k, xpeer(xs_n - 1) if way == 0 else xpeer(1))
        copy = remote(
            ref, ref, sems.at[2, k], rsems.at[2, k], east if way == 0 else west
        )
        copy.start()
        started.append(copy)

    def settle(part, sems, rsems, k):
        arrive(part, rsems, sems, 1 - k % 2, k)
        arrive(part, rsems, sems, 2, k)

    def step_a(k):
        if k == 1:
            kk = 1 - h
            for step in (0, 1):
                if step == 1:
                    ref = tok.at[kk, c, :, own_cols]
                    remote(ref, ref, yd_s.at[0], yd_r.at[kk], partner).wait_recv()
                    which = kk
                else:
                    which = h
                ref = tok.at[which, c, :, own_cols]
                for way, dev in ((0, east), (1, west)):
                    copy = remote(ref, ref, tx_s.at[way, which], tx_r.at[way, which], dev)
                    copy.start()
                    started.append(copy)
        elif k > 1:
            ref = tok.at[k, c, :, own_cols]
            remote(ref, ref, yd_s.at[0], yd_r.at[k], partner).wait_recv()
            spread(tok_part, tx_s, tx_r, k)

    def step_b(k):
        relay(tok_part, tx_s, tx_r, k)

    def step_c(k):
        settle(tok_part, tx_s, tx_r, k)
        ref = tok.at[k, c]
        copy = remote(ref, ref, tc_s.at[k], tc_r.at[k], partner)
        copy.start()
        started.append(copy)

    def step_e(j):
        for k in (2 * j, 2 * j + 1):
            ref = tok.at[k, 1 - c]
            remote(ref, ref, tc_s.at[k], tc_r.at[k], partner).wait_recv()
        if j == 0:
            weights[0].wait()
            weights[1].wait()
        rows = tok[2 * j : 2 * j + 2].reshape(2 * CORES * erow, width)
        pre = jnp.dot(rows, w_gu[...], preferred_element_type=f32)
        gate, up = pre[:, :fx], pre[:, fx:]
        hidden = (gate / (1.0 + jnp.exp(-gate)) * up).astype(bf16)
        cols = pl.ds(pl.multiple_of(x * fx, fx), fx)
        hid[2 * j : 2 * j + 2, :, :, cols] = hidden.reshape(2, CORES, erow, fx)
        for k in (2 * j, 2 * j + 1):
            spread(hid_part, hx_s, hx_r, k)

    def step_f(k):
        relay(hid_part, hx_s, hx_r, k)

    def step_g(j):
        for k in (2 * j, 2 * j + 1):
            settle(hid_part, hx_s, hx_r, k)
        if j == 0:
            weights[2].wait()
        rows = hid[2 * j : 2 * j + 2].reshape(2 * CORES * erow, hid.shape[3])
        part = jnp.dot(rows, w_dn[...], preferred_element_type=f32)
        part = part.reshape(2, CORES, erow, dx)
        acc[...] = part
        psend[2 * j : 2 * j + 2] = part.astype(bf16)
        copy = remote(
            psend.at[pl.ds(2 * j, 2), 1 - c],
            precv.at[pl.ds(2 * j, 2)],
            pc_s.at[j],
            pc_r.at[j],
            partner,
        )
        copy.start()
        started.append(copy)
        return copy

    def step_i(j, copy):
        copy.wait_recv()
        total = acc[:, c] + precv[2 * j : 2 * j + 2].astype(f32)
        half[j] = total
        qsend[2 * j : 2 * j + 2] = total.astype(bf16)
        other = at(z, y + 1 - 2 * h, c, x)
        copy = remote(
            qsend.at[2 * j + 1 - h], qrecv.at[j], qy_s.at[j], qy_r.at[j], other
        )
        copy.start()
        started.append(copy)
        return copy

    def step_j(j, copy):
        copy.wait_recv()
        done = (half[j, h] + qrecv[j].astype(f32)).astype(bf16)
        if j == 0:
            yback[pair] = done
            return
        fsend[j] = done
        back = lax.rem(y + ys_n + j * (2 * h - 1), ys_n)
        copy = remote(fsend.at[j], yback.at[pair], fy_s.at[j], fy_r.at[j], at(z, back, c, x))
        copy.start()
        started.append(copy)
        backs.append(copy)

    backs = []
    nj = pairs
    pend_g, pend_i = {}, {}

    def branch_core():
        for copy in bz:
            copy.wait_recv()
        copy = remote(bw.at[:, :, :, c], bw.at[:, :, :, c], bc_s.at[0], bc_r.at[0], partner)
        copy.start()
        started.append(copy)

    def branch_dense():
        ref = bw.at[:, :, :, 1 - c]
        remote(ref, ref, bc_s.at[0], bc_r.at[0], partner).wait_recv()
        whole_in = bw[0].reshape(width, bw.shape[5])
        pre = jnp.dot(normed[...], whole_in, preferred_element_type=f32)
        hb = (pre / (1.0 + jnp.exp(-pre))).astype(bf16)
        for xx in range(xs_n):
            zpart = zs_n // xs_n if zs_n >= xs_n else 0
            if zpart:
                wo = bw[1, xx * zpart : (xx + 1) * zpart].reshape(dx, bw.shape[5])
            else:
                wo = bw[1].reshape(width, bw.shape[5])[xx * dx : (xx + 1) * dx]
            term = lax.dot_general(hb, wo, (((1,), (1,)), ((), ())), preferred_element_type=f32)
            bterm[xx] = term.astype(bf16)

    bx = []

    def branch_send():
        for r in range(1, xs_n):
            xt = xpeer(r)
            copy = remote(bterm.at[xt], bgot.at[r], bx_s.at[r], bx_r.at[r], at(z, y, c, xt))
            copy.start()
            bx.append(copy)

    for k in (0, 1):
        step_a(k)
    for j in range(nj):
        nxt = (2 * j + 2, 2 * j + 3)
        for k in (2 * j, 2 * j + 1):
            step_b(k)
        if j + 1 < nj:
            for k in nxt:
                step_a(k)
        for k in (2 * j, 2 * j + 1):
            step_c(k)
        if j == min(1, nj - 1):
            branch_core()
        step_e(j)
        if j > 0:
            for k in (2 * j - 2, 2 * j - 1):
                step_f(k)
    branch_dense()
    last = nj - 1
    for k in (2 * last, 2 * last + 1):
        step_f(k)
    branch_send()
    for j in range(nj):
        pend = step_g(j)
        pend = step_i(j, pend)
        step_j(j, pend)

    tlane = lax.broadcasted_iota(jnp.int32, (slots, pairs * erow), 0).astype(f32)
    trow = lax.broadcasted_iota(jnp.int32, (slots, pairs * erow), 1).astype(f32)
    unpack = jnp.where(row_target(trow) == tlane, 1.0, 0.0).astype(bf16)
    for copy in backs:
        copy.wait_recv()
    back_rows = yback[...].reshape(pairs * erow, dx)
    zout = jnp.dot(unpack, back_rows, preferred_element_type=f32).astype(bf16)
    zback[...] = zout.reshape(zs_n, zrow, dx)
    zb = []
    for r in range(1, zs_n):
        zt = zpeer(r)
        copy = remote(zback.at[zt], zgot.at[z], zb_s.at[r], zb_r.at[r], at(zt, y, c, x))
        copy.start()
        zb.append(copy)
    zgot[z] = zback[z]

    for copy in bx:
        copy.wait_recv()
    share = bterm[x].astype(f32)
    for r in range(1, xs_n):
        share = share + bgot[r].astype(f32)
    share = share * branch_weight
    q0, q1 = positions(routes[:, 0:1], routes[:, 1:2], 1)
    slane = lax.broadcasted_iota(jnp.int32, (rows_tok, slots), 1).astype(f32)
    g0 = jnp.where(slane == q0, 1.0, 0.0).astype(bf16)
    g1 = jnp.where(slane == q1, 1.0, 0.0).astype(bf16)
    diff = scores[:, 0:1] - scores[:, 1:2]
    w0, w1 = sigmoid(diff), sigmoid(-diff)
    for copy in zb:
        copy.wait_recv()
    got = zgot[...].reshape(slots, dx)
    r0 = jnp.dot(g0, got, preferred_element_type=f32)
    r1 = jnp.dot(g1, got, preferred_element_type=f32)
    out[...] = (w0 * r0 + w1 * r1 + share).astype(out.dtype)

    for copy in zd + by + yd + bz + started + bx + zb:
        copy.wait_send()


def on_device(
    cores_z,
    cores_y,
    tokens,
    norm_gain,
    routes,
    route_scores,
    expert_gate,
    expert_up,
    expert_down,
    branch_in,
    branch_out,
    branch_gate,
):
    zs_n, ys_n = cores_z, cores_y
    xs_n = lax.axis_size("tp")
    rows_tok, width = tokens.shape
    experts = zs_n * ys_n // 2
    cap = 5 * rows_tok * routes.shape[1] // (4 * experts)
    pairs = ys_n // 2
    dx = width // xs_n
    fx = expert_gate.shape[2]
    fg = expert_down.shape[1]
    zrow = round_up(pairs * cap, 16)
    erow = round_up(zs_n * cap, 16)
    brow = branch_in.shape[0]
    bcol = branch_in.shape[1]
    bweights = jnp.stack([branch_in, branch_out.T])
    bf16, f32 = jnp.bfloat16, jnp.float32
    vm = lambda shape, dtype=bf16: pltpu.VMEM(shape, dtype)
    sem = lambda *shape: pltpu.SemaphoreType.DMA(shape)
    scratch = [
        vm((rows_tok, width)),
        vm((zs_n, zrow, dx)),
        vm((zs_n, zrow, dx)),
        vm((pairs, erow, dx)),
        vm((ys_n, CORES, erow, width)),
        vm((width, 2 * fx)),
        vm((fg, dx)),
        vm((ys_n, CORES, erow, fg)),
        vm((2, CORES, erow, dx), f32),
        vm((ys_n, CORES, erow, dx)),
        vm((ys_n, erow, dx)),
        vm((pairs, 2, erow, dx), f32),
        vm((ys_n, erow, dx)),
        vm((pairs, erow, dx)),
        vm((pairs, erow, dx)),
        vm((pairs, erow, dx)),
        vm((zs_n, zrow, dx)),
        vm((zs_n, zrow, dx)),
        vm((2, zs_n, ys_n, CORES, brow, bcol)),
        vm((xs_n, rows_tok, dx)),
        vm((xs_n, rows_tok, dx)),
        sem(3),
        sem(zs_n),
        sem(zs_n),
        sem(ys_n),
        sem(ys_n),
        sem(3, ys_n),
        sem(3, ys_n),
        sem(ys_n),
        sem(ys_n),
        sem(3, ys_n),
        sem(3, ys_n),
        sem(pairs),
        sem(pairs),
        sem(pairs),
        sem(pairs),
        sem(pairs),
        sem(pairs),
        sem(zs_n),
        sem(zs_n),
        sem(ys_n),
        sem(ys_n),
        sem(zs_n),
        sem(zs_n),
        sem(1),
        sem(1),
        sem(xs_n),
        sem(xs_n),
    ]
    in_vmem = pl.BlockSpec(memory_space=pltpu.VMEM)
    in_hbm = pl.BlockSpec(memory_space=pl.ANY)
    return pl.pallas_call(
        functools.partial(layer_kernel, zs_n, ys_n, xs_n, cap),
        out_shape=jax.ShapeDtypeStruct((rows_tok, dx), bf16),
        in_specs=[in_vmem] * 7 + [in_hbm] * 3,
        out_specs=in_vmem,
        scratch_shapes=scratch,
        compiler_params=pltpu.CompilerParams(
            collective_id=0, has_side_effects=True, vmem_limit_bytes=60 * 1024 * 1024
        ),
        name="routed_layer",
    )(
        tokens,
        norm_gain.reshape(1, -1),
        routes,
        routes.T,
        route_scores,
        branch_gate.reshape(1, -1),
        bweights,
        expert_gate,
        expert_up,
        expert_down,
    )


def solution(mesh, z_y=None):
    ep = mesh.shape["ep"]
    zs_n, ys_n = z_y or (8, ep // (8 * CORES))
    in_specs = (
        P("ep", None),
        P(),
        P("ep", None),
        P("ep", None),
        P("ep", None, "tp"),
        P("ep", None, "tp"),
        P("ep", None, "tp"),
        P("ep", "tp"),
        P("tp", "ep"),
        P(),
    )
    return jax.shard_map(
        functools.partial(on_device, zs_n, ys_n),
        mesh=mesh,
        in_specs=in_specs,
        out_specs=P("ep", "tp"),
        check_vma=False,
    )
```

```python
import functools

import jax
import jax.numpy as jnp
from jax import lax
from jax.experimental import pallas as pl
from jax.experimental.pallas import tpu as pltpu
from jax.sharding import PartitionSpec as P

NORM_EPSILON = 1e-06
GROUP = 4
CORES = 2
MESH_ID = pl.DeviceIdType.MESH


def round_up(n, m):
    return (n + m - 1) // m * m


def sigmoid(v):
    return 1.0 / (1.0 + jnp.exp(-v))


def floor_div(v, n):
    return jnp.floor((v + 0.5) * (1.0 / n))


def layer_kernel(
    zs_n,
    ys_n,
    xs_n,
    cap,
    tokens,
    gain,
    routes_t,
    scores_t,
    bgate,
    b_in,
    b_out,
    w_gate,
    w_up,
    w_down,
    out,
    normed,
    zsend_a,
    zsend_b,
    zrecv_a,
    zrecv_b,
    ysend,
    tok,
    w_gu,
    w_dn,
    hid,
    acc,
    psend,
    precv,
    half,
    qsend,
    qrecv,
    fsend,
    yback,
    zback_a,
    zback_b,
    zgot_a,
    zgot_b,
    bw,
    bterm,
    bgot,
    local_sem,
    za_s,
    za_r,
    zd_s,
    zd_r,
    yd_s,
    yd_r,
    tx_s,
    tx_r,
    tc_s,
    tc_r,
    hx_s,
    hx_r,
    pc_s,
    pc_r,
    qy_s,
    qy_r,
    fy_s,
    fy_r,
    zb_s,
    zb_r,
    zc_s,
    zc_r,
    by_s,
    by_r,
    bz_s,
    bz_r,
    bc_s,
    bc_r,
    bx_s,
    bx_r,
):
    f32, bf16 = jnp.float32, jnp.bfloat16
    ep = lax.axis_index("ep")
    x = lax.axis_index("tp")
    c = lax.rem(ep, CORES)
    y = lax.rem(ep // CORES, ys_n)
    z = ep // (CORES * ys_n)
    pairs = ys_n // 2
    pair = y // 2
    h = lax.rem(y, 2)
    hops = [0] + list(range(2, pairs)) + [1]
    rows_tok, width = tokens.shape
    dx = width // xs_n
    fx = w_gate.shape[2]
    experts = zs_n * pairs
    arow = zsend_a.shape[1]
    brow = zsend_b.shape[1]
    a_slots, b_slots = zs_n * arow, zs_n * brow
    erow = ysend.shape[1]
    mates = pairs - 1

    def at(z_, y_, c_, x_):
        return ((z_ * ys_n + y_) * CORES + c_, x_)

    def zpeer(r):
        return lax.rem(z + r, zs_n)

    def ypeer(r):
        return lax.rem(y + r, ys_n)

    def xpeer(r):
        return lax.rem(x + r, xs_n)

    def remote(src, dst, s, r, dev):
        return pltpu.make_async_remote_copy(
            src_ref=src, dst_ref=dst, send_sem=s, recv_sem=r, device_id=dev, device_id_type=MESH_ID
        )

    barrier = pltpu.get_barrier_semaphore()
    peers = [at(zpeer(r), y, c, x) for r in range(1, zs_n)]
    peers += [at(z, ypeer(r), c, x) for r in range(1, ys_n)]
    peers += [at(z, y, c, xpeer(r)) for r in range(1, xs_n)]
    peers += [at(z, y, 1 - c, x)]
    for dev in peers:
        pl.semaphore_signal(barrier, inc=1, device_id=dev, device_id_type=MESH_ID)

    weights = [
        pltpu.make_async_copy(w_gate.at[0], w_gu.at[:, pl.ds(0, fx)], local_sem.at[0]),
        pltpu.make_async_copy(w_up.at[0], w_gu.at[:, pl.ds(fx, fx)], local_sem.at[1]),
        pltpu.make_async_copy(w_down.at[0], w_dn, local_sem.at[2]),
    ]
    for copy in weights:
        copy.start()

    tf = tokens[...].astype(f32)
    scaled = lax.rsqrt(jnp.sum(tf * tf, axis=-1, keepdims=True) * (1.0 / width) + NORM_EPSILON)
    nf = (tf * scaled * gain[...]).astype(bf16)
    normed[...] = nf

    ids = lax.broadcasted_iota(jnp.int32, (experts, rows_tok), 0)
    sq = (rows_tok, rows_tok)
    sq_a = lax.broadcasted_iota(jnp.int32, sq, 0)
    sq_b = lax.broadcasted_iota(jnp.int32, sq, 1)
    chosen = [jnp.where(ids == routes_t[r : r + 1, :], 1.0, 0.0) for r in (0, 1)]
    earlier = jnp.where(sq_a < sq_b, 1.0, 0.0).astype(bf16)
    ranks = jnp.dot((chosen[0] + chosen[1]).astype(bf16), earlier, preferred_element_type=f32)
    go, come = [], []
    for r in (0, 1):
        rank = jnp.sum(chosen[r] * ranks, axis=0, keepdims=True)
        e = routes_t[r : r + 1, :].astype(f32)
        zz = floor_div(e, pairs)
        v = (e - zz * pairs - pair.astype(f32)) * (1 - 2 * h).astype(f32) + pairs
        rel = jnp.where(v >= pairs, v - pairs, v)
        go.append(
            rank
            + jnp.where(rel < 0.5, zz * arow, a_slots + zz * brow + (rel - 1.0) * cap)
        )
        come.append(
            rank
            + jnp.where(rel < mates - 0.5, zz * brow + rel * cap, b_slots + zz * arow)
        )
    srow = lax.broadcasted_iota(jnp.int32, (a_slots + b_slots, rows_tok), 0).astype(f32)
    pick = jnp.where((srow == go[0]) | (srow == go[1]), 1.0, 0.0).astype(bf16)
    own_cols = pl.ds(pl.multiple_of(x * dx, dx), dx)
    packed = jnp.dot(pick, normed[:, own_cols], preferred_element_type=f32).astype(bf16)
    zsend_a[...] = packed[:a_slots].reshape(zs_n, arow, dx)
    zsend_b[...] = packed[a_slots:].reshape(zs_n, brow, dx)

    pl.semaphore_wait(barrier, len(peers))

    za, zd, by = [], [], []
    near = sorted(range(1, zs_n), key=lambda r: min(r, zs_n - r))
    for src, dst, ss, rs, kept in (
        (zsend_a, zrecv_a, za_s, za_r, za),
        (zsend_b, zrecv_b, zd_s, zd_r, zd),
    ):
        for copy in za:
            copy.wait_send()
        for r in near:
            zt = zpeer(r)
            copy = remote(src.at[zt], dst.at[z], ss.at[r], rs.at[r], at(zt, y, c, x))
            copy.start()
            kept.append(copy)
    for r in range(1, ys_n):
        for w, part in enumerate((b_in, b_out)):
            copy = remote(
                part, bw.at[w, z, y, c], by_s.at[w, r], by_r.at[w, r], at(z, ypeer(r), c, x)
            )
            copy.start()
            by.append(copy)
    bw[0, z, y, c] = b_in[...]
    bw[1, z, y, c] = b_out[...]
    zrecv_a[z] = zsend_a[z]
    zrecv_b[z] = zsend_b[z]

    bsum = jnp.sum(normed[...].astype(f32) * bgate[...], axis=-1, keepdims=True)
    branch_weight = sigmoid(bsum)

    def row_target(q, step):
        pp = floor_div(q, erow)
        rem = q - pp * erow
        zz = floor_div(rem, cap)
        return jnp.where(zz < zs_n, zz * step + pp * cap + (rem - zz * cap), -1.0)

    def permutation(rows, slots, step):
        q = lax.broadcasted_iota(jnp.int32, (rows, slots), 0).astype(f32)
        t = lax.broadcasted_iota(jnp.int32, (rows, slots), 1).astype(f32)
        return jnp.where(row_target(q, step) == t, 1.0, 0.0).astype(bf16)

    def unpermutation(rows, slots, step):
        q = lax.broadcasted_iota(jnp.int32, (slots, rows), 1).astype(f32)
        t = lax.broadcasted_iota(jnp.int32, (slots, rows), 0).astype(f32)
        return jnp.where(row_target(q, step) == t, 1.0, 0.0).astype(bf16)

    east, west = at(z, y, c, xpeer(1)), at(z, y, c, xpeer(xs_n - 1))
    partner = at(z, y, 1 - c, x)
    mate = at(z, y + 1 - 2 * h, c, x)
    started, backs, bz, bx, backs_z = [], [], [], [], []
    pending = {}

    def begin(copy):
        copy.start()
        started.append(copy)
        return copy

    def tok_part(k, xx):
        return tok.at[k, c, :, pl.ds(pl.multiple_of(xx * dx, dx), dx)]

    def hid_part(k, xx):
        return hid.at[k, :, :, pl.ds(pl.multiple_of(xx * fx, fx), fx)]

    def spread(part, sems, rsems, k):
        for way, dev in ((0, east), (1, west)):
            begin(remote(part(k, x), part(k, x), sems.at[way, k], rsems.at[way, k], dev))

    def arrive(part, rsems, sems, way, k):
        ref = part(k, x)
        remote(ref, ref, sems.at[way, k], rsems.at[way, k], east).wait_recv()

    def relay(part, sems, rsems, k):
        way = k % 2
        arrive(part, rsems, sems, way, k)
        ref = part(k, xpeer(xs_n - 1) if way == 0 else xpeer(1))
        begin(remote(ref, ref, sems.at[2, k], rsems.at[2, k], east if way == 0 else west))

    def settle(part, sems, rsems, k):
        arrive(part, rsems, sems, 1 - k % 2, k)
        arrive(part, rsems, sems, 2, k)

    def y_wait(k):
        ref = tok.at[k, c, :, own_cols]
        remote(ref, ref, yd_s.at[0], yd_r.at[k], mate).wait_recv()

    def both(i):
        return (2 * i, 2 * i + 1)

    def own_pair():
        with jax.named_scope("za_wait"):
            for copy in za:
                copy.wait_recv()
        first = permutation(erow, a_slots, arow)
        moved = jnp.dot(first, zrecv_a[...].reshape(a_slots, dx), preferred_element_type=f32)
        tok[h, c, :, own_cols] = moved.astype(bf16)
        ref = tok.at[h, c, :, own_cols]
        begin(remote(ref, ref, yd_s.at[0], yd_r.at[h], mate))
        spread(tok_part, tx_s, tx_r, h)
        with jax.named_scope("y_wait_mate"):
            y_wait(1 - h)
        spread(tok_part, tx_s, tx_r, 1 - h)

    def other_pairs():
        rest = permutation(mates * erow, b_slots, brow)
        with jax.named_scope("zb_wait"):
            for copy in zd:
                copy.wait_recv()
        moved = jnp.dot(rest, zrecv_b[...].reshape(b_slots, dx), preferred_element_type=f32)
        ysend[...] = moved.astype(bf16).reshape(mates, erow, dx)
        for i in range(1, pairs):
            pt = lax.rem(pair + pairs + i * (1 - 2 * h), pairs)
            k = 2 * i + lax.rem(h + hops[i], 2)
            for hh in (0, 1):
                begin(
                    remote(
                        ysend.at[i - 1],
                        tok.at[k, c, :, own_cols],
                        yd_s.at[2 * i + hh],
                        yd_r.at[k],
                        at(z, 2 * pt + hh, c, x),
                    )
                )

    def branch_planes():
        for copy in by:
            copy.wait_recv()
        for r in range(1, zs_n):
            part = bw.at[:, z, :, c]
            copy = remote(part, part, bz_s.at[r], bz_r.at[r], at(zpeer(r), y, c, x))
            copy.start()
            bz.append(copy)

    def step_a(i):
        for k in both(i):
            with jax.named_scope(f"a_wait{k}"):
                y_wait(k)
            spread(tok_part, tx_s, tx_r, k)

    def step_b(i):
        for k in both(i):
            with jax.named_scope(f"b_relay{k}"):
                relay(tok_part, tx_s, tx_r, k)

    def step_c(i):
        for k in both(i):
            with jax.named_scope(f"c_settle{k}"):
                settle(tok_part, tx_s, tx_r, k)
            ref = tok.at[k, c]
            begin(remote(ref, ref, tc_s.at[k], tc_r.at[k], partner))

    def step_e(i):
        with jax.named_scope(f"e_wait{i}"):
            for k in both(i):
                ref = tok.at[k, 1 - c]
                remote(ref, ref, tc_s.at[k], tc_r.at[k], partner).wait_recv()
            if i == 0:
                weights[0].wait()
                weights[1].wait()
        with jax.named_scope(f"e_dot{i}"):
            rows = tok[2 * i : 2 * i + 2].reshape(2 * CORES * erow, width)
            pre = jnp.dot(rows, w_gu[...], preferred_element_type=f32)
            gate, up = pre[:, :fx], pre[:, fx:]
            hidden = (gate / (1.0 + jnp.exp(-gate)) * up).astype(bf16)
            cols = pl.ds(pl.multiple_of(x * fx, fx), fx)
            hid[2 * i : 2 * i + 2, :, :, cols] = hidden.reshape(2, CORES, erow, fx)
        for k in both(i):
            spread(hid_part, hx_s, hx_r, k)

    def step_f(i):
        for k in both(i):
            with jax.named_scope(f"f_relay{k}"):
                relay(hid_part, hx_s, hx_r, k)

    def step_g(i):
        for k in both(i):
            with jax.named_scope(f"g_settle{k}"):
                settle(hid_part, hx_s, hx_r, k)
        if i == 0:
            weights[2].wait()
        with jax.named_scope(f"g_dot{i}"):
            rows = hid[2 * i : 2 * i + 2].reshape(2 * CORES * erow, hid.shape[3])
            part = jnp.dot(rows, w_dn[...], preferred_element_type=f32)
            part = part.reshape(2, CORES, erow, dx)
            acc[...] = part
            psend[2 * i : 2 * i + 2] = part.astype(bf16)
        two = pl.ds(2 * i, 2)
        pending["g", i] = begin(
            remote(psend.at[two, 1 - c], precv.at[two], pc_s.at[i], pc_r.at[i], partner)
        )

    def step_i(i):
        with jax.named_scope(f"i_wait{i}"):
            pending["g", i].wait_recv()
        total = acc[:, c] + precv[2 * i : 2 * i + 2].astype(f32)
        half[i] = total
        qsend[2 * i : 2 * i + 2] = total.astype(bf16)
        pending["i", i] = begin(
            remote(qsend.at[2 * i + 1 - h], qrecv.at[i], qy_s.at[i], qy_r.at[i], mate)
        )

    def step_j(i):
        with jax.named_scope(f"j_wait{i}"):
            pending["i", i].wait_recv()
        done = (half[i, h] + qrecv[i].astype(f32)).astype(bf16)
        if i == 0:
            yback[0] = done
            return
        fsend[i] = done
        back = lax.rem(y + ys_n + hops[i] * (2 * h - 1), ys_n)
        pending["j", i] = begin(
            remote(fsend.at[i], yback.at[i], fy_s.at[i], fy_r.at[i], at(z, back, c, x))
        )

    def z_return(group):
        if group == 0:
            perm = unpermutation(mates * erow, b_slots, brow)
        else:
            perm = unpermutation(erow, a_slots, arow)
        with jax.named_scope(f"back_wait{group}"):
            for i in range(1, mates) if group == 0 else (mates,):
                pending["j", i].wait_recv()
        if group == 0:
            rows = yback[0:mates].reshape(mates * erow, dx)
            send, got, ss, rs = zback_a, zgot_a, zb_s, zb_r
        else:
            rows = yback[mates]
            send, got, ss, rs = zback_b, zgot_b, zc_s, zc_r
        moved = jnp.dot(perm, rows, preferred_element_type=f32).astype(bf16)
        send[...] = moved.reshape(send.shape)
        kept = []
        for r in near:
            zt = zpeer(r)
            copy = remote(send.at[zt], got.at[z], ss.at[r], rs.at[r], at(zt, y, c, x))
            copy.start()
            kept.append(copy)
        got[z] = send[z]
        backs_z.extend(kept)
        return kept

    def branch_core():
        with jax.named_scope("bz_wait"):
            for copy in bz:
                copy.wait_recv()
        begin(remote(bw.at[:, :, :, c], bw.at[:, :, :, c], bc_s.at[0], bc_r.at[0], partner))

    def branch_dense():
        ref = bw.at[:, :, :, 1 - c]
        remote(ref, ref, bc_s.at[0], bc_r.at[0], partner).wait_recv()
        whole_in = bw[0].reshape(width, bw.shape[5])
        pre = jnp.dot(normed[...], whole_in, preferred_element_type=f32)
        hb = (pre / (1.0 + jnp.exp(-pre))).astype(bf16)
        for xx in range(xs_n):
            zpart = zs_n // xs_n if zs_n >= xs_n else 0
            if zpart:
                wo = bw[1, xx * zpart : (xx + 1) * zpart].reshape(dx, bw.shape[5])
            else:
                wo = bw[1].reshape(width, bw.shape[5])[xx * dx : (xx + 1) * dx]
            term = lax.dot_general(hb, wo, (((1,), (1,)), ((), ())), preferred_element_type=f32)
            bterm[xx] = term.astype(bf16)

    def branch_send():
        for r in range(1, xs_n):
            xt = xpeer(r)
            copy = remote(bterm.at[xt], bgot.at[r], bx_s.at[r], bx_r.at[r], at(z, y, c, xt))
            copy.start()
            bx.append(copy)

    last = pairs - 1
    own_pair()
    other_pairs()
    step_b(0)
    step_c(0)
    branch_planes()
    step_e(0)
    if pairs == 4:
        order = ("a1", "f0", "b1", "a2", "g0", "c1", "a3", "i0", "e1", "b2", "j0", "core", "b3", "c2", "e2", "f1", "c3", "e3", "dense", "g1", "f2", "i1", "j1", "f3", "g2", "i2", "g3", "send", "j2", "i3")
    else:
        order = ("a1", "f0", "b1", "g0", "c1", "i0", "e1", "j0", "core", "dense", "f1", "g1", "send", "i1")
    steps = dict(a=step_a, b=step_b, c=step_c, e=step_e, f=step_f, g=step_g, i=step_i, j=step_j)
    others = dict(core=branch_core, dense=branch_dense, send=branch_send)
    for item in order:
        if item in others:
            others[item]()
        else:
            steps[item[0]](int(item[1]))
    step_j(last)
    kept_a = z_return(0)
    kept_b = z_return(1)

    diff = scores_t[0:1, :] - scores_t[1:2, :]
    mixes = []
    for d in (diff, -diff):
        row = jnp.broadcast_to(sigmoid(d), sq)
        mixes.append(jnp.sum(jnp.where(sq_a == sq_b, row, 0.0), axis=1, keepdims=True))

    def combine(low, slots, got):
        t = lax.broadcasted_iota(jnp.int32, (slots, rows_tok), 0).astype(f32) + low
        rows = got[...].reshape(slots, dx)
        total = None
        for r in (0, 1):
            g = jnp.where(t == come[r], 1.0, 0.0).astype(bf16)
            term = lax.dot_general(g, rows, (((0,), (0,)), ((), ())), preferred_element_type=f32)
            total = mixes[r] * term if total is None else total + mixes[r] * term
        return total

    with jax.named_scope("bx_wait"):
        for copy in bx:
            copy.wait_recv()
    share = bterm[x].astype(f32)
    for r in range(1, xs_n):
        share = share + bgot[r].astype(f32)
    share = share * branch_weight
    with jax.named_scope("kept_a"):
        for copy in kept_a:
            copy.wait_recv()
    share = share + combine(0.0, b_slots, zgot_a)
    with jax.named_scope("kept_b"):
        for copy in kept_b:
            copy.wait_recv()
    out[...] = (share + combine(b_slots * 1.0, a_slots, zgot_b)).astype(out.dtype)

    with jax.named_scope("send_wait"):
        for copy in zd + by + bz + started + bx + backs_z:
            copy.wait_send()


def on_device(
    cores_z,
    cores_y,
    tokens,
    norm_gain,
    routes,
    route_scores,
    expert_gate,
    expert_up,
    expert_down,
    branch_in,
    branch_out,
    branch_gate,
):
    zs_n, ys_n = cores_z, cores_y
    xs_n = lax.axis_size("tp")
    rows_tok, width = tokens.shape
    experts = zs_n * ys_n // 2
    cap = 5 * rows_tok * routes.shape[1] // (4 * experts)
    pairs = ys_n // 2
    dx = width // xs_n
    fx = expert_gate.shape[2]
    fg = expert_down.shape[1]
    arow = round_up(cap, 16)
    brow = round_up((pairs - 1) * cap, 16)
    erow = round_up(zs_n * cap, 16)
    bpart = branch_in.shape
    bf16, f32 = jnp.bfloat16, jnp.float32
    vm = lambda shape, dtype=bf16: pltpu.VMEM(shape, dtype)
    sem = lambda *shape: pltpu.SemaphoreType.DMA(shape)
    scratch = [
        vm((rows_tok, width)),
        vm((zs_n, arow, dx)),
        vm((zs_n, brow, dx)),
        vm((zs_n, arow, dx)),
        vm((zs_n, brow, dx)),
        vm((pairs - 1, erow, dx)),
        vm((ys_n, CORES, erow, width)),
        vm((width, 2 * fx)),
        vm((fg, dx)),
        vm((ys_n, CORES, erow, fg)),
        vm((2, CORES, erow, dx), f32),
        vm((ys_n, CORES, erow, dx)),
        vm((ys_n, erow, dx)),
        vm((pairs, 2, erow, dx), f32),
        vm((ys_n, erow, dx)),
        vm((pairs, erow, dx)),
        vm((pairs, erow, dx)),
        vm((pairs, erow, dx)),
        vm((zs_n, brow, dx)),
        vm((zs_n, arow, dx)),
        vm((zs_n, brow, dx)),
        vm((zs_n, arow, dx)),
        vm((2, zs_n, ys_n, CORES, *bpart)),
        vm((xs_n, rows_tok, dx)),
        vm((xs_n, rows_tok, dx)),
        sem(3),
        sem(zs_n),
        sem(zs_n),
        sem(zs_n),
        sem(zs_n),
        sem(ys_n),
        sem(ys_n),
        sem(3, ys_n),
        sem(3, ys_n),
        sem(ys_n),
        sem(ys_n),
        sem(3, ys_n),
        sem(3, ys_n),
        sem(pairs),
        sem(pairs),
        sem(pairs),
        sem(pairs),
        sem(pairs),
        sem(pairs),
        sem(zs_n),
        sem(zs_n),
        sem(zs_n),
        sem(zs_n),
        sem(2, ys_n),
        sem(2, ys_n),
        sem(zs_n),
        sem(zs_n),
        sem(1),
        sem(1),
        sem(xs_n),
        sem(xs_n),
    ]
    in_vmem = pl.BlockSpec(memory_space=pltpu.VMEM)
    in_hbm = pl.BlockSpec(memory_space=pl.ANY)
    return pl.pallas_call(
        functools.partial(layer_kernel, zs_n, ys_n, xs_n, cap),
        out_shape=jax.ShapeDtypeStruct((rows_tok, dx), bf16),
        in_specs=[in_vmem] * 7 + [in_hbm] * 3,
        out_specs=in_vmem,
        scratch_shapes=scratch,
        compiler_params=pltpu.CompilerParams(
            collective_id=0, has_side_effects=True, vmem_limit_bytes=60 * 1024 * 1024
        ),
        name="routed_layer",
    )(
        tokens,
        norm_gain.reshape(1, -1),
        routes.T,
        route_scores.T,
        branch_gate.reshape(1, -1),
        branch_in,
        branch_out.T,
        expert_gate,
        expert_up,
        expert_down,
    )


def solution(mesh, z_y=None):
    ep = mesh.shape["ep"]
    zs_n, ys_n = z_y or (8, ep // (8 * CORES))
    in_specs = (
        P("ep", None),
        P(),
        P("ep", None),
        P("ep", None),
        P("ep", None, "tp"),
        P("ep", None, "tp"),
        P("ep", None, "tp"),
        P("ep", "tp"),
        P("tp", "ep"),
        P(),
    )
    return jax.shard_map(
        functools.partial(on_device, zs_n, ys_n),
        mesh=mesh,
        in_specs=in_specs,
        out_specs=P("ep", "tp"),
        check_vma=False,
    )
```

```python
import functools

import jax
import jax.numpy as jnp
from jax import lax
from jax.experimental import pallas as pl
from jax.experimental.pallas import tpu as pltpu
from jax.sharding import PartitionSpec as P

NORM_EPSILON = 1e-06
GROUP = 4
CORES = 2
MESH_ID = pl.DeviceIdType.MESH


def round_up(n, m):
    return (n + m - 1) // m * m


def sigmoid(v):
    return 1.0 / (1.0 + jnp.exp(-v))


def floor_div(v, n):
    return jnp.floor((v + 0.5) * (1.0 / n))


def return_groups(pairs):
    return [[0, 1], [2], [3]] if pairs == 4 else [[i] for i in range(pairs)]


def layer_kernel(
    zs_n,
    ys_n,
    xs_n,
    cap,
    tokens,
    gain,
    routes_t,
    scores_t,
    bgate,
    b_in,
    b_out,
    w_gate,
    w_up,
    w_down,
    out,
    normed,
    zsend_a,
    zsend_b,
    zrecv_a,
    zrecv_b,
    ysend,
    tok,
    w_gu,
    w_dn,
    hid,
    acc,
    psend,
    precv,
    half,
    qrecv,
    fsend,
    yback,
    zback,
    zgot,
    bw,
    bterm,
    bgot,
    local_sem,
    za_s,
    za_r,
    zd_s,
    zd_r,
    yd_s,
    yd_r,
    tx_s,
    tx_r,
    tc_s,
    tc_r,
    hx_s,
    hx_r,
    pc_s,
    pc_r,
    qy_s,
    qy_r,
    fy_s,
    fy_r,
    zb_s,
    zb_r,
    by_s,
    by_r,
    bz_s,
    bz_r,
    bc_s,
    bc_r,
    bx_s,
    bx_r,
):
    f32, bf16 = jnp.float32, jnp.bfloat16
    ep = lax.axis_index("ep")
    x = lax.axis_index("tp")
    c = lax.rem(ep, CORES)
    y = lax.rem(ep // CORES, ys_n)
    z = ep // (CORES * ys_n)
    pairs = ys_n // 2
    pair = y // 2
    h = lax.rem(y, 2)
    hops = [0] + list(range(2, pairs)) + [1]
    rows_tok, width = tokens.shape
    dx = width // xs_n
    fx = w_gate.shape[2]
    experts = zs_n * pairs
    arow = zsend_a.shape[1]
    brow = zsend_b.shape[1]
    a_slots, b_slots = zs_n * arow, zs_n * brow
    erow = ysend.shape[1]
    mates = pairs - 1
    far = hops.index(pairs - 1)
    groups = return_groups(pairs)
    g_rows = [round_up(len(g) * cap, 16) for g in groups]
    g_low = [zs_n * sum(g_rows[:n]) for n in range(len(groups))]

    def at(z_, y_, c_, x_):
        return ((z_ * ys_n + y_) * CORES + c_, x_)

    def zpeer(r):
        return lax.rem(z + r, zs_n)

    def ypeer(r):
        return lax.rem(y + r, ys_n)

    def xpeer(r):
        return lax.rem(x + r, xs_n)

    def remote(src, dst, s, r, dev):
        return pltpu.make_async_remote_copy(
            src_ref=src, dst_ref=dst, send_sem=s, recv_sem=r, device_id=dev, device_id_type=MESH_ID
        )

    barrier = pltpu.get_barrier_semaphore()
    peers = [at(zpeer(r), y, c, x) for r in range(1, zs_n)]
    peers += [at(z, ypeer(r), c, x) for r in range(1, ys_n)]
    peers += [at(z, y, c, xpeer(r)) for r in range(1, xs_n)]
    peers += [at(z, y, 1 - c, x)]
    for dev in peers:
        pl.semaphore_signal(barrier, inc=1, device_id=dev, device_id_type=MESH_ID)

    weights = [
        pltpu.make_async_copy(w_gate.at[0], w_gu.at[:, pl.ds(0, fx)], local_sem.at[0]),
        pltpu.make_async_copy(w_up.at[0], w_gu.at[:, pl.ds(fx, fx)], local_sem.at[1]),
        pltpu.make_async_copy(w_down.at[0], w_dn, local_sem.at[2]),
    ]
    for copy in weights:
        copy.start()

    tf = tokens[...].astype(f32)
    scaled = lax.rsqrt(jnp.sum(tf * tf, axis=-1, keepdims=True) * (1.0 / width) + NORM_EPSILON)
    nf = (tf * scaled * gain[...]).astype(bf16)
    normed[...] = nf

    ids = lax.broadcasted_iota(jnp.int32, (experts, rows_tok), 0)
    sq = (rows_tok, rows_tok)
    sq_a = lax.broadcasted_iota(jnp.int32, sq, 0)
    sq_b = lax.broadcasted_iota(jnp.int32, sq, 1)
    chosen = [jnp.where(ids == routes_t[r : r + 1, :], 1.0, 0.0) for r in (0, 1)]
    earlier = jnp.where(sq_a < sq_b, 1.0, 0.0).astype(bf16)
    ranks = jnp.dot((chosen[0] + chosen[1]).astype(bf16), earlier, preferred_element_type=f32)
    go, come = [], []
    for r in (0, 1):
        rank = jnp.sum(chosen[r] * ranks, axis=0, keepdims=True)
        e = routes_t[r : r + 1, :].astype(f32)
        zz = floor_div(e, pairs)
        v = (e - zz * pairs - pair.astype(f32)) * (1 - 2 * h).astype(f32) + pairs
        rel = jnp.where(v >= pairs, v - pairs, v)
        go.append(
            rank
            + jnp.where(rel < 0.5, zz * arow, a_slots + zz * brow + (rel - 1.0) * cap)
        )
        place = 0.0
        for group, n_rows, low in zip(groups, g_rows, g_low):
            spot = low + zz * n_rows + (rel - group[0]) * cap
            place = spot if group[0] == 0 else jnp.where(rel > group[0] - 0.5, spot, place)
        come.append(rank + place)
    srow = lax.broadcasted_iota(jnp.int32, (a_slots + b_slots, rows_tok), 0).astype(f32)
    pick = jnp.where((srow == go[0]) | (srow == go[1]), 1.0, 0.0).astype(bf16)
    own_cols = pl.ds(pl.multiple_of(x * dx, dx), dx)
    packed = jnp.dot(pick, normed[:, own_cols], preferred_element_type=f32).astype(bf16)
    zsend_a[...] = packed[:a_slots].reshape(zs_n, arow, dx)
    zsend_b[...] = packed[a_slots:].reshape(zs_n, brow, dx)

    pl.semaphore_wait(barrier, len(peers))

    za, zd, by = [], [], []
    near = sorted(range(1, zs_n), key=lambda r: min(r, zs_n - r))
    for src, dst, ss, rs, kept in (
        (zsend_a, zrecv_a, za_s, za_r, za),
        (zsend_b, zrecv_b, zd_s, zd_r, zd),
    ):
        for copy in za:
            copy.wait_send()
        for r in near:
            zt = zpeer(r)
            copy = remote(src.at[zt], dst.at[z], ss.at[r], rs.at[r], at(zt, y, c, x))
            copy.start()
            kept.append(copy)
    for r in range(1, ys_n):
        for w, part in enumerate((b_in, b_out)):
            copy = remote(
                part, bw.at[w, z, y, c], by_s.at[w, r], by_r.at[w, r], at(z, ypeer(r), c, x)
            )
            copy.start()
            by.append(copy)
    bw[0, z, y, c] = b_in[...]
    bw[1, z, y, c] = b_out[...]
    zrecv_a[z] = zsend_a[z]
    zrecv_b[z] = zsend_b[z]

    bsum = jnp.sum(normed[...].astype(f32) * bgate[...], axis=-1, keepdims=True)
    branch_weight = sigmoid(bsum)

    def row_target(q, step):
        pp = floor_div(q, erow)
        rem = q - pp * erow
        zz = floor_div(rem, cap)
        return jnp.where(zz < zs_n, zz * step + pp * cap + (rem - zz * cap), -1.0)

    def permutation(rows, slots, step):
        q = lax.broadcasted_iota(jnp.int32, (rows, slots), 0).astype(f32)
        t = lax.broadcasted_iota(jnp.int32, (rows, slots), 1).astype(f32)
        return jnp.where(row_target(q, step) == t, 1.0, 0.0).astype(bf16)

    def unpermutation(rows, slots, step):
        q = lax.broadcasted_iota(jnp.int32, (slots, rows), 1).astype(f32)
        t = lax.broadcasted_iota(jnp.int32, (slots, rows), 0).astype(f32)
        return jnp.where(row_target(q, step) == t, 1.0, 0.0).astype(bf16)

    east, west = at(z, y, c, xpeer(1)), at(z, y, c, xpeer(xs_n - 1))
    partner = at(z, y, 1 - c, x)
    mate = at(z, y + 1 - 2 * h, c, x)
    started, bz, bx, backs_z, returned = [], [], [], [], []
    pending = {}

    def begin(copy):
        copy.start()
        started.append(copy)
        return copy

    def tok_part(k, xx):
        return tok.at[k, c, :, pl.ds(pl.multiple_of(xx * dx, dx), dx)]

    def hid_part(k, xx):
        return hid.at[k, :, :, pl.ds(pl.multiple_of(xx * fx, fx), fx)]

    def spread(part, sems, rsems, k):
        for way, dev in ((0, east), (1, west)):
            begin(remote(part(k, x), part(k, x), sems.at[way, k], rsems.at[way, k], dev))

    def arrive(part, rsems, sems, way, k):
        ref = part(k, x)
        remote(ref, ref, sems.at[way, k], rsems.at[way, k], east).wait_recv()

    def relay(part, sems, rsems, k):
        way = k % 2
        arrive(part, rsems, sems, way, k)
        ref = part(k, xpeer(xs_n - 1) if way == 0 else xpeer(1))
        begin(remote(ref, ref, sems.at[2, k], rsems.at[2, k], east if way == 0 else west))

    def settle(part, sems, rsems, k):
        arrive(part, rsems, sems, 1 - k % 2, k)
        arrive(part, rsems, sems, 2, k)

    def y_wait(k):
        ref = tok.at[k, c, :, own_cols]
        remote(ref, ref, yd_s.at[0], yd_r.at[k], mate).wait_recv()

    def both(i):
        return (2 * i, 2 * i + 1)

    def own_pair():
        with jax.named_scope("za_wait"):
            for copy in za:
                copy.wait_recv()
        first = permutation(erow, a_slots, arow)
        moved = jnp.dot(first, zrecv_a[...].reshape(a_slots, dx), preferred_element_type=f32)
        tok[h, c, :, own_cols] = moved.astype(bf16)
        ref = tok.at[h, c, :, own_cols]
        begin(remote(ref, ref, yd_s.at[0], yd_r.at[h], mate))
        spread(tok_part, tx_s, tx_r, h)
        with jax.named_scope("y_wait_mate"):
            y_wait(1 - h)
        spread(tok_part, tx_s, tx_r, 1 - h)

    def other_pairs():
        rest = permutation(mates * erow, b_slots, brow)
        with jax.named_scope("zb_wait"):
            for copy in zd:
                copy.wait_recv()
        moved = jnp.dot(rest, zrecv_b[...].reshape(b_slots, dx), preferred_element_type=f32)
        ysend[...] = moved.astype(bf16).reshape(mates, erow, dx)
        for i in range(1, pairs):
            pt = lax.rem(pair + pairs + i * (1 - 2 * h), pairs)
            k = 2 * i + lax.rem(h + hops[i], 2)
            near_chip = lax.rem(h + hops[i], 2)
            for n, hh in enumerate((near_chip, 1 - near_chip)):
                if i == far and n == 1:
                    break
                begin(
                    remote(
                        ysend.at[i - 1],
                        tok.at[k, c, :, own_cols],
                        yd_s.at[2 * i + n],
                        yd_r.at[k],
                        at(z, 2 * pt + hh, c, x),
                    )
                )

    def branch_planes():
        for copy in by:
            copy.wait_recv()
        for r in range(1, zs_n):
            part = bw.at[:, z, :, c]
            copy = remote(part, part, bz_s.at[r], bz_r.at[r], at(zpeer(r), y, c, x))
            copy.start()
            bz.append(copy)

    def step_k(k):
        with jax.named_scope(f"a_wait{k}"):
            y_wait(k)
        spread(tok_part, tx_s, tx_r, k)

    def step_a(i):
        for k in both(i):
            step_k(k)

    def step_n(i):
        mine = 2 * i + h
        with jax.named_scope(f"far_wait{i}"):
            y_wait(mine)
        ref = tok.at[mine, c, :, own_cols]
        begin(remote(ref, ref, yd_s.at[2 * i + 1], yd_r.at[mine], mate))
        spread(tok_part, tx_s, tx_r, mine)

    def step_m(i):
        with jax.named_scope(f"far_mate{i}"):
            y_wait(2 * i + 1 - h)
        spread(tok_part, tx_s, tx_r, 2 * i + 1 - h)

    def step_b(i):
        for k in both(i):
            with jax.named_scope(f"b_relay{k}"):
                relay(tok_part, tx_s, tx_r, k)

    def step_c(i):
        for k in both(i):
            with jax.named_scope(f"c_settle{k}"):
                settle(tok_part, tx_s, tx_r, k)
            ref = tok.at[k, c]
            begin(remote(ref, ref, tc_s.at[k], tc_r.at[k], partner))

    def step_e(i):
        with jax.named_scope(f"e_wait{i}"):
            for k in both(i):
                ref = tok.at[k, 1 - c]
                remote(ref, ref, tc_s.at[k], tc_r.at[k], partner).wait_recv()
            if i == 0:
                weights[0].wait()
                weights[1].wait()
        with jax.named_scope(f"e_dot{i}"):
            rows = tok[2 * i : 2 * i + 2].reshape(2 * CORES * erow, width)
            pre = jnp.dot(rows, w_gu[...], preferred_element_type=f32)
            gate, up = pre[:, :fx], pre[:, fx:]
            hidden = (gate / (1.0 + jnp.exp(-gate)) * up).astype(bf16)
            cols = pl.ds(pl.multiple_of(x * fx, fx), fx)
            hid[2 * i : 2 * i + 2, :, :, cols] = hidden.reshape(2, CORES, erow, fx)
        for k in both(i):
            spread(hid_part, hx_s, hx_r, k)

    def step_f(i):
        for k in both(i):
            with jax.named_scope(f"f_relay{k}"):
                relay(hid_part, hx_s, hx_r, k)

    def step_g(i):
        for k in both(i):
            with jax.named_scope(f"g_settle{k}"):
                settle(hid_part, hx_s, hx_r, k)
        if i == 0:
            weights[2].wait()
        with jax.named_scope(f"g_dot{i}"):
            rows = hid[2 * i : 2 * i + 2].reshape(2 * CORES * erow, hid.shape[3])
            part = jnp.dot(rows, w_dn[...], preferred_element_type=f32)
            part = part.reshape(2, CORES, erow, dx)
            acc[...] = part
            psend[2 * i : 2 * i + 2] = part.astype(bf16)
        two = pl.ds(2 * i, 2)
        pending["g", i] = begin(
            remote(psend.at[two, 1 - c], precv.at[two], pc_s.at[i], pc_r.at[i], partner)
        )

    def step_i(i):
        with jax.named_scope(f"i_wait{i}"):
            pending["g", i].wait_recv()
        total = acc[:, c] + precv[2 * i : 2 * i + 2].astype(f32)
        fsend[2 * i : 2 * i + 2] = total.astype(bf16)
        if i == 0:
            yback[0, h] = fsend[h]
            begin(remote(fsend.at[1 - h], yback.at[0, h], fy_s.at[0], fy_r.at[0, h], mate))
            return
        if i == far:
            half[...] = total
            copy = remote(fsend.at[2 * i + 1 - h], qrecv, qy_s.at[0], qy_r.at[0], mate)
            pending["i", i] = begin(copy)
            return
        for side in (0, 1):
            way = hops[i] + 1 if side else ys_n - hops[i]
            back = at(z, lax.rem(2 * pair + way, ys_n), c, x)
            k = 2 * i + side
            begin(remote(fsend.at[k], yback.at[i, h], fy_s.at[k], fy_r.at[i, h], back))

    def step_j(i):
        with jax.named_scope(f"j_wait{i}"):
            pending["i", i].wait_recv()
        fsend[2 * i + h] = (half[h] + qrecv[...].astype(f32)).astype(bf16)
        back = at(z, lax.rem(y + ys_n + hops[i] * (2 * h - 1), ys_n), c, x)
        k = 2 * i + h
        begin(remote(fsend.at[k], yback.at[i, 0], fy_s.at[2 * i], fy_r.at[i, 0], back))

    def back_wait(i, hh):
        ref = yback.at[i, hh]
        remote(ref, ref, fy_s.at[0], fy_r.at[i, hh], mate).wait_recv()

    def z_return(n):
        group, step = groups[n], g_rows[n]
        many, slots = len(group) * erow, zs_n * step
        perm = unpermutation(many, slots, step)
        with jax.named_scope(f"back_wait{n}"):
            for i in group:
                if i == 0:
                    back_wait(0, 1 - h)
                elif i == far:
                    back_wait(i, 0)
                else:
                    back_wait(i, 0)
                    back_wait(i, 1)
        moved = 0.0
        for hh in (0,) if group == [far] else (0, 1):
            rows = yback[group[0] : group[-1] + 1, hh].reshape(many, dx)
            moved = moved + jnp.dot(perm, rows, preferred_element_type=f32)
        base = sum(g_rows[:n])
        zback[:, base : base + step] = moved.astype(bf16).reshape(zs_n, step, dx)
        rows = pl.ds(base, step)
        kept = []
        for r in near:
            zt = zpeer(r)
            copy = remote(
                zback.at[zt, rows], zgot.at[z, rows], zb_s.at[n, r], zb_r.at[n, r], at(zt, y, c, x)
            )
            copy.start()
            kept.append(copy)
        zgot[z, base : base + step] = zback[z, base : base + step]
        backs_z.extend(kept)
        returned.append((n, kept))

    def branch_core():
        with jax.named_scope("bz_wait"):
            for copy in bz:
                copy.wait_recv()
        begin(remote(bw.at[:, :, :, c], bw.at[:, :, :, c], bc_s.at[0], bc_r.at[0], partner))

    def branch_dense():
        ref = bw.at[:, :, :, 1 - c]
        remote(ref, ref, bc_s.at[0], bc_r.at[0], partner).wait_recv()
        whole_in = bw[0].reshape(width, bw.shape[5])
        pre = jnp.dot(normed[...], whole_in, preferred_element_type=f32)
        hb = (pre / (1.0 + jnp.exp(-pre))).astype(bf16)
        for xx in range(xs_n):
            zpart = zs_n // xs_n if zs_n >= xs_n else 0
            if zpart:
                wo = bw[1, xx * zpart : (xx + 1) * zpart].reshape(dx, bw.shape[5])
            else:
                wo = bw[1].reshape(width, bw.shape[5])[xx * dx : (xx + 1) * dx]
            term = lax.dot_general(hb, wo, (((1,), (1,)), ((), ())), preferred_element_type=f32)
            bterm[xx] = term.astype(bf16)

    def branch_send():
        for r in range(1, xs_n):
            xt = xpeer(r)
            copy = remote(bterm.at[xt], bgot.at[r], bx_s.at[r], bx_r.at[r], at(z, y, c, xt))
            copy.start()
            bx.append(copy)

    own_pair()
    other_pairs()
    if pairs == 4:
        order = ("b0", "k2", "c0", "planes", "e0", "k3", "n2", "f0", "b1", "m2", "a3", "g0", "c1", "b2", "i0", "e1", "core", "b3", "c2", "e2", "c3", "f1", "e3", "g1", "f2", "i1", "f3", "dense", "g2", "i2", "g3", "send", "z0", "i3", "j2", "z2", "z1")
    else:
        order = ("b0", "n1", "m1", "c0", "planes", "e0", "f0", "b1", "g0", "c1", "i0", "e1", "core", "dense", "f1", "g1", "send", "i1", "j1", "z0", "z1")
    steps = dict(a=step_a, b=step_b, c=step_c, e=step_e, f=step_f, g=step_g, i=step_i, j=step_j)
    steps.update(k=step_k, z=z_return, n=step_n, m=step_m)
    others = dict(planes=branch_planes, core=branch_core, dense=branch_dense, send=branch_send)
    for item in order:
        if item in others:
            others[item]()
        else:
            steps[item[0]](int(item[1]))

    diff = scores_t[0:1, :] - scores_t[1:2, :]
    mixes = []
    for d in (diff, -diff):
        row = jnp.broadcast_to(sigmoid(d), sq)
        mixes.append(jnp.sum(jnp.where(sq_a == sq_b, row, 0.0), axis=1, keepdims=True))

    def combine(n):
        slots = zs_n * g_rows[n]
        base = sum(g_rows[:n])
        t = lax.broadcasted_iota(jnp.int32, (slots, rows_tok), 0).astype(f32) + 1.0 * g_low[n]
        rows = zgot[:, base : base + g_rows[n]].reshape(slots, dx)
        total = None
        for r in (0, 1):
            g = jnp.where(t == come[r], 1.0, 0.0).astype(bf16)
            term = lax.dot_general(g, rows, (((0,), (0,)), ((), ())), preferred_element_type=f32)
            total = mixes[r] * term if total is None else total + mixes[r] * term
        return total

    with jax.named_scope("bx_wait"):
        for copy in bx:
            copy.wait_recv()
    share = bterm[x].astype(f32)
    for r in range(1, xs_n):
        share = share + bgot[r].astype(f32)
    share = share * branch_weight
    for n, kept in returned:
        with jax.named_scope(f"kept{n}"):
            for copy in kept:
                copy.wait_recv()
        share = share + combine(n)
    out[...] = share.astype(out.dtype)

    with jax.named_scope("send_wait"):
        for copy in zd + by + bz + started + bx + backs_z:
            copy.wait_send()


def on_device(
    cores_z,
    cores_y,
    tokens,
    norm_gain,
    routes,
    route_scores,
    expert_gate,
    expert_up,
    expert_down,
    branch_in,
    branch_out,
    branch_gate,
):
    zs_n, ys_n = cores_z, cores_y
    xs_n = lax.axis_size("tp")
    rows_tok, width = tokens.shape
    experts = zs_n * ys_n // 2
    cap = 5 * rows_tok * routes.shape[1] // (4 * experts)
    pairs = ys_n // 2
    dx = width // xs_n
    fx = expert_gate.shape[2]
    fg = expert_down.shape[1]
    arow = round_up(cap, 16)
    brow = round_up((pairs - 1) * cap, 16)
    erow = round_up(zs_n * cap, 16)
    back_rows = sum(round_up(len(g) * cap, 16) for g in return_groups(pairs))
    bpart = branch_in.shape
    bf16, f32 = jnp.bfloat16, jnp.float32
    vm = lambda shape, dtype=bf16: pltpu.VMEM(shape, dtype)
    sem = lambda *shape: pltpu.SemaphoreType.DMA(shape)
    scratch = [
        vm((rows_tok, width)),
        vm((zs_n, arow, dx)),
        vm((zs_n, brow, dx)),
        vm((zs_n, arow, dx)),
        vm((zs_n, brow, dx)),
        vm((pairs - 1, erow, dx)),
        vm((ys_n, CORES, erow, width)),
        vm((width, 2 * fx)),
        vm((fg, dx)),
        vm((ys_n, CORES, erow, fg)),
        vm((2, CORES, erow, dx), f32),
        vm((ys_n, CORES, erow, dx)),
        vm((ys_n, erow, dx)),
        vm((2, erow, dx), f32),
        vm((erow, dx)),
        vm((ys_n, erow, dx)),
        vm((pairs, 2, erow, dx)),
        vm((zs_n, back_rows, dx)),
        vm((zs_n, back_rows, dx)),
        vm((2, zs_n, ys_n, CORES, *bpart)),
        vm((xs_n, rows_tok, dx)),
        vm((xs_n, rows_tok, dx)),
        sem(3),
        sem(zs_n),
        sem(zs_n),
        sem(zs_n),
        sem(zs_n),
        sem(ys_n),
        sem(ys_n),
        sem(3, ys_n),
        sem(3, ys_n),
        sem(ys_n),
        sem(ys_n),
        sem(3, ys_n),
        sem(3, ys_n),
        sem(pairs),
        sem(pairs),
        sem(1),
        sem(1),
        sem(ys_n),
        sem(pairs, 2),
        sem(pairs, zs_n),
        sem(pairs, zs_n),
        sem(2, ys_n),
        sem(2, ys_n),
        sem(zs_n),
        sem(zs_n),
        sem(1),
        sem(1),
        sem(xs_n),
        sem(xs_n),
    ]
    in_vmem = pl.BlockSpec(memory_space=pltpu.VMEM)
    in_hbm = pl.BlockSpec(memory_space=pl.ANY)
    return pl.pallas_call(
        functools.partial(layer_kernel, zs_n, ys_n, xs_n, cap),
        out_shape=jax.ShapeDtypeStruct((rows_tok, dx), bf16),
        in_specs=[in_vmem] * 7 + [in_hbm] * 3,
        out_specs=in_vmem,
        scratch_shapes=scratch,
        compiler_params=pltpu.CompilerParams(
            collective_id=0, has_side_effects=True, vmem_limit_bytes=60 * 1024 * 1024
        ),
        name="routed_layer",
    )(
        tokens,
        norm_gain.reshape(1, -1),
        routes.T,
        route_scores.T,
        branch_gate.reshape(1, -1),
        branch_in,
        branch_out.T,
        expert_gate,
        expert_up,
        expert_down,
    )


def solution(mesh, z_y=None):
    ep = mesh.shape["ep"]
    zs_n, ys_n = z_y or (8, ep // (8 * CORES))
    in_specs = (
        P("ep", None),
        P(),
        P("ep", None),
        P("ep", None),
        P("ep", None, "tp"),
        P("ep", None, "tp"),
        P("ep", None, "tp"),
        P("ep", "tp"),
        P("tp", "ep"),
        P(),
    )
    return jax.shard_map(
        functools.partial(on_device, zs_n, ys_n),
        mesh=mesh,
        in_specs=in_specs,
        out_specs=P("ep", "tp"),
        check_vma=False,
    )
```

```python
import functools

import jax
import jax.numpy as jnp
from jax import lax
from jax.experimental import pallas as pl
from jax.experimental.pallas import tpu as pltpu
from jax.sharding import PartitionSpec as P

NORM_EPSILON = 1e-06
GROUP = 4
CORES = 2
MESH_ID = pl.DeviceIdType.MESH


def round_up(n, m):
    return (n + m - 1) // m * m


def sigmoid(v):
    return 1.0 / (1.0 + jnp.exp(-v))


def floor_div(v, n):
    return jnp.floor((v + 0.5) * (1.0 / n))


def return_groups(pairs):
    return [[0, 1], [2], [3]] if pairs == 4 else [[i] for i in range(pairs)]


def layer_kernel(
    zs_n,
    ys_n,
    xs_n,
    cap,
    tokens,
    gain,
    routes_t,
    scores_t,
    bgate,
    b_in,
    b_out,
    w_gate,
    w_up,
    w_down,
    out,
    normed,
    zsend,
    zrecv,
    wsend,
    wrecv,
    ysend,
    tok,
    w_gu,
    w_dn,
    hid,
    acc,
    psend,
    precv,
    half,
    qrecv,
    fsend,
    yback,
    zback,
    zgot,
    bw,
    bterm,
    bgot,
    local_sem,
    zd_s,
    zd_r,
    yd_s,
    yd_r,
    tx_s,
    tx_r,
    tc_s,
    tc_r,
    hx_s,
    hx_r,
    pc_s,
    pc_r,
    qy_s,
    qy_r,
    fy_s,
    fy_r,
    zb_s,
    zb_r,
    by_s,
    by_r,
    bz_s,
    bz_r,
    bc_s,
    bc_r,
    bx_s,
    bx_r,
):
    f32, bf16 = jnp.float32, jnp.bfloat16
    ep = lax.axis_index("ep")
    x = lax.axis_index("tp")
    c = lax.rem(ep, CORES)
    y = lax.rem(ep // CORES, ys_n)
    z = ep // (CORES * ys_n)
    pairs = ys_n // 2
    pair = y // 2
    h = lax.rem(y, 2)
    hops = list(range(1, pairs)) + [0]
    last = pairs - 1
    offset = [last] + list(range(1, last)) + [0]
    rows_tok, width = tokens.shape
    dx = width // xs_n
    fx = w_gate.shape[2]
    experts = zs_n * pairs
    arow = zsend.shape[2]
    slots = zs_n * arow
    erow = ysend.shape[1]
    far = hops.index(last)
    groups = return_groups(pairs)
    g_rows = [round_up(len(g) * cap, 16) for g in groups]
    g_low = [zs_n * sum(g_rows[:n]) for n in range(len(groups))]

    def at(z_, y_, c_, x_):
        return ((z_ * ys_n + y_) * CORES + c_, x_)

    def zpeer(r):
        return lax.rem(z + r, zs_n)

    def ypeer(r):
        return lax.rem(y + r, ys_n)

    def xpeer(r):
        return lax.rem(x + r, xs_n)

    def remote(src, dst, s, r, dev):
        return pltpu.make_async_remote_copy(
            src_ref=src, dst_ref=dst, send_sem=s, recv_sem=r, device_id=dev, device_id_type=MESH_ID
        )

    barrier = pltpu.get_barrier_semaphore()
    peers = [at(zpeer(r), y, c, x) for r in range(1, zs_n)]
    peers += [at(z, ypeer(r), c, x) for r in range(1, ys_n)]
    peers += [at(z, y, c, xpeer(r)) for r in range(1, xs_n)]
    peers += [at(z, y, 1 - c, x)]
    for dev in peers:
        pl.semaphore_signal(barrier, inc=1, device_id=dev, device_id_type=MESH_ID)

    weights = [
        pltpu.make_async_copy(w_gate.at[0], w_gu.at[:, pl.ds(0, fx)], local_sem.at[0]),
        pltpu.make_async_copy(w_up.at[0], w_gu.at[:, pl.ds(fx, fx)], local_sem.at[1]),
        pltpu.make_async_copy(w_down.at[0], w_dn, local_sem.at[2]),
    ]
    for copy in weights:
        copy.start()

    tf = tokens[...].astype(f32)
    scaled = lax.rsqrt(jnp.sum(tf * tf, axis=-1, keepdims=True) * (1.0 / width) + NORM_EPSILON)
    nf = (tf * scaled * gain[...]).astype(bf16)
    normed[...] = nf

    ids = lax.broadcasted_iota(jnp.int32, (experts, rows_tok), 0)
    sq = (rows_tok, rows_tok)
    sq_a = lax.broadcasted_iota(jnp.int32, sq, 0)
    sq_b = lax.broadcasted_iota(jnp.int32, sq, 1)
    chosen = [jnp.where(ids == routes_t[r : r + 1, :], 1.0, 0.0) for r in (0, 1)]
    earlier = jnp.where(sq_a < sq_b, 1.0, 0.0).astype(bf16)
    ranks = jnp.dot((chosen[0] + chosen[1]).astype(bf16), earlier, preferred_element_type=f32)
    go, come = [], []
    for r in (0, 1):
        rank = jnp.sum(chosen[r] * ranks, axis=0, keepdims=True)
        e = routes_t[r : r + 1, :].astype(f32)
        zz = floor_div(e, pairs)
        v = (e - zz * pairs - pair.astype(f32)) * (1 - 2 * h).astype(f32) + pairs
        rel = jnp.where(v >= pairs, v - pairs, v)
        rel = jnp.where(rel < 0.5, 1.0 * last, jnp.where(rel > last - 0.5, 0.0, rel))
        go.append(rank + rel * slots + zz * arow)
        place = 0.0
        for group, n_rows, low in zip(groups, g_rows, g_low):
            spot = low + zz * n_rows + (rel - group[0]) * cap
            place = spot if group[0] == 0 else jnp.where(rel > group[0] - 0.5, spot, place)
        come.append(rank + place)
    srow = lax.broadcasted_iota(jnp.int32, (pairs * slots, rows_tok), 0).astype(f32)
    pick = jnp.where((srow == go[0]) | (srow == go[1]), 1.0, 0.0).astype(bf16)
    own_cols = pl.ds(pl.multiple_of(x * dx, dx), dx)
    packed = jnp.dot(pick[: last * slots], normed[:, own_cols], preferred_element_type=f32)
    zsend[...] = packed.astype(bf16).reshape(last, zs_n, arow, dx)

    pl.semaphore_wait(barrier, len(peers))

    zd, by = {}, []
    near = sorted(range(1, zs_n), key=lambda r: min(r, zs_n - r))

    def z_send(i):
        src, dst = (wsend, wrecv) if i == last else (zsend.at[i], zrecv.at[i])
        zd[i] = []
        for r in near:
            zt = zpeer(r)
            copy = remote(src.at[zt], dst.at[z], zd_s.at[i], zd_r.at[i], at(zt, y, c, x))
            copy.start()
            zd[i].append(copy)

    def zd_all(i):
        ref = wrecv if i == last else zrecv.at[i]
        ref = ref.at[pl.ds(0, zs_n - 1)]
        return remote(ref, ref, zd_s.at[i], zd_r.at[i], at(z, y, 1 - c, x))

    z_send(0)
    for i in range(last):
        zrecv[i, z] = zsend[i, z]
    wide = jnp.dot(pick[last * slots :], normed[...], preferred_element_type=f32)
    wsend[...] = wide.astype(bf16).reshape(zs_n, arow, width)
    wrecv[z] = wsend[z]
    if near:
        zd_all(0).wait_send()
    z_send(1)
    for r in near:
        for w, part in enumerate((b_in, b_out)):
            copy = remote(
                part, bw.at[w, z, y, c], by_s.at[0], by_r.at[0], at(zpeer(r), y, c, x)
            )
            copy.start()
            by.append(copy)
    bw[0, z, y, c] = b_in[...]
    bw[1, z, y, c] = b_out[...]

    bsum = jnp.sum(normed[...].astype(f32) * bgate[...], axis=-1, keepdims=True)
    branch_weight = sigmoid(bsum)

    def row_target(q, step):
        pp = floor_div(q, erow)
        rem = q - pp * erow
        zz = floor_div(rem, cap)
        return jnp.where(zz < zs_n, zz * step + pp * cap + (rem - zz * cap), -1.0)

    def permutation(rows, slots, step):
        q = lax.broadcasted_iota(jnp.int32, (rows, slots), 0).astype(f32)
        t = lax.broadcasted_iota(jnp.int32, (rows, slots), 1).astype(f32)
        return jnp.where(row_target(q, step) == t, 1.0, 0.0).astype(bf16)

    def unpermutation(rows, slots, step):
        q = lax.broadcasted_iota(jnp.int32, (slots, rows), 1).astype(f32)
        t = lax.broadcasted_iota(jnp.int32, (slots, rows), 0).astype(f32)
        return jnp.where(row_target(q, step) == t, 1.0, 0.0).astype(bf16)

    east, west = at(z, y, c, xpeer(1)), at(z, y, c, xpeer(xs_n - 1))
    partner = at(z, y, 1 - c, x)
    mate = at(z, y + 1 - 2 * h, c, x)
    started, bz, bx, backs_z, returned = [], [], [], [], []
    pending = {}

    def begin(copy):
        copy.start()
        started.append(copy)
        return copy

    def tok_part(k, xx):
        return tok.at[k, c, :, pl.ds(pl.multiple_of(xx * dx, dx), dx)]

    def hid_part(k, xx):
        return hid.at[k, :, :, pl.ds(pl.multiple_of(xx * fx, fx), fx)]

    def spread(part, sems, rsems, k):
        for way, dev in ((0, east), (1, west)):
            begin(remote(part(k, x), part(k, x), sems.at[0], rsems.at[way, k], dev))

    def arrive(part, rsems, sems, way, k):
        ref = part(k, x)
        remote(ref, ref, sems.at[0], rsems.at[way, k], east).wait_recv()

    def relay(part, sems, rsems, k):
        way = lax.rem(k, 2)
        arrive(part, rsems, sems, way, k)
        ref = part(k, xpeer(xs_n - 1 - 2 * way))
        dev = at(z, y, c, xpeer(1 + 2 * way))
        begin(remote(ref, ref, sems.at[0], rsems.at[2, k], dev))

    def settle(part, sems, rsems, k):
        arrive(part, rsems, sems, 1 - k % 2, k)
        arrive(part, rsems, sems, 2, k)

    def y_wait(k):
        ref = tok.at[k, c, :, own_cols]
        remote(ref, ref, yd_s.at[0], yd_r.at[k], mate).wait_recv()

    def both(i):
        return (2 * i, 2 * i + 1)

    def step_d(i):
        perm = permutation(erow, slots, arow)
        with jax.named_scope(f"z_wait{i}"):
            if near:
                zd_all(i).wait_recv()
        moved = jnp.dot(perm, zrecv[i].reshape(slots, dx), preferred_element_type=f32)
        ysend[i] = moved.astype(bf16)
        pt = lax.rem(pair + pairs + offset[i] * (1 - 2 * h), pairs)
        near_chip = lax.rem(h + hops[i], 2)
        k = 2 * i + near_chip
        for n, hh in enumerate((near_chip, 1 - near_chip)):
            if i == far and n == 1:
                break
            dst = tok.at[k, c, :, own_cols]
            dev = at(z, 2 * pt + hh, c, x)
            begin(remote(ysend.at[i], dst, yd_s.at[0], yd_r.at[k], dev))
        if i + 2 <= last:
            z_send(i + 2)

    def to_partner(k, ref):
        begin(remote(ref, ref, tc_s.at[0], tc_r.at[k], partner))

    def step_o(part):
        mine = 2 * last + h
        if part == 1:
            perm = permutation(erow, slots, arow)
            with jax.named_scope("z_wait_wide"):
                if near:
                    zd_all(last).wait_recv()
            moved = jnp.dot(perm, wrecv[...].reshape(slots, width), preferred_element_type=f32)
            tok[mine, c] = moved.astype(bf16)
            ref = tok.at[mine, c]
            begin(remote(ref, ref, yd_s.at[0], yd_r.at[mine], mate))
            to_partner(mine, ref)
            return
        ref = tok.at[2 * last + 1 - h, c]
        with jax.named_scope("wide_mate"):
            remote(ref, ref, yd_s.at[0], yd_r.at[2 * last + 1 - h], mate).wait_recv()
        to_partner(2 * last + 1 - h, ref)

    def by_all():
        ref = bw.at[:, 0, pl.ds(0, zs_n - 1), 0]
        return remote(ref, ref, by_s.at[0], by_r.at[0], partner)

    def bz_all():
        ref = bw.at[:, :, pl.ds(0, ys_n - 1), 0]
        return remote(ref, ref, bz_s.at[0], bz_r.at[0], partner)

    def bx_all():
        ref = bgot.at[pl.ds(0, xs_n - 1)]
        return remote(ref, ref, bx_s.at[0], bx_r.at[0], partner)

    def branch_planes():
        if near:
            by_all().wait_recv()
        for r in range(1, ys_n):
            part = bw.at[:, :, y, c]
            copy = remote(part, part, bz_s.at[0], bz_r.at[0], at(z, ypeer(r), c, x))
            copy.start()
            bz.append(copy)

    def step_n(i):
        mine = 2 * i + h
        with jax.named_scope(f"n_wait{i}"):
            y_wait(mine)
        if i == far:
            ref = tok.at[mine, c, :, own_cols]
            begin(remote(ref, ref, yd_s.at[0], yd_r.at[mine], mate))
        spread(tok_part, tx_s, tx_r, mine)
        to_partner(mine, tok_part(mine, x))

    def step_m(i):
        with jax.named_scope(f"m_wait{i}"):
            y_wait(2 * i + 1 - h)
        k = 2 * i + 1 - h
        spread(tok_part, tx_s, tx_r, k)
        to_partner(k, tok_part(k, x))

    def step_b(i):
        for n, k in enumerate((2 * i + h, 2 * i + 1 - h)):
            with jax.named_scope(f"b_relay{i}_{n}"):
                relay(tok_part, tx_s, tx_r, k)
            to_partner(k, tok_part(k, xpeer(xs_n - 1 - 2 * lax.rem(k, 2))))

    def step_c(i):
        for k in both(i):
            way = k % 2
            with jax.named_scope(f"c_settle{k}"):
                arrive(tok_part, tx_r, tx_s, 1 - way, k)
            to_partner(k, tok_part(k, xpeer(1 + 2 * way)))
        for k in both(i):
            with jax.named_scope(f"c_last{k}"):
                arrive(tok_part, tx_r, tx_s, 2, k)
            to_partner(k, tok_part(k, xpeer(2)))

    def step_e(i):
        with jax.named_scope(f"e_wait{i}"):
            for k in both(i):
                ref = tok.at[k, 1 - c]
                remote(ref, ref, tc_s.at[0], tc_r.at[k], partner).wait_recv()
            while len(weights) > 1:
                weights.pop(0).wait()
        with jax.named_scope(f"e_dot{i}"):
            rows = tok[2 * i : 2 * i + 2].reshape(2 * CORES * erow, width)
            pre = jnp.dot(rows, w_gu[...], preferred_element_type=f32)
            gate, up = pre[:, :fx], pre[:, fx:]
            hidden = (gate / (1.0 + jnp.exp(-gate)) * up).astype(bf16)
            cols = pl.ds(pl.multiple_of(x * fx, fx), fx)
            hid[2 * i : 2 * i + 2, :, :, cols] = hidden.reshape(2, CORES, erow, fx)
        for k in both(i):
            spread(hid_part, hx_s, hx_r, k)

    def step_f(i):
        for k in both(i):
            with jax.named_scope(f"f_relay{k}"):
                relay(hid_part, hx_s, hx_r, k)

    def step_g(i):
        for k in both(i):
            with jax.named_scope(f"g_settle{k}"):
                settle(hid_part, hx_s, hx_r, k)
        while weights:
            weights.pop(0).wait()
        with jax.named_scope(f"g_dot{i}"):
            rows = hid[2 * i : 2 * i + 2].reshape(2 * CORES * erow, hid.shape[3])
            part = jnp.dot(rows, w_dn[...], preferred_element_type=f32)
            part = part.reshape(2, CORES, erow, dx)
            acc[...] = part
            psend[2 * i : 2 * i + 2] = part.astype(bf16)
        two = pl.ds(2 * i, 2)
        pending["g", i] = begin(
            remote(psend.at[two, 1 - c], precv.at[two], pc_s.at[0], pc_r.at[i], partner)
        )

    def step_i(i):
        with jax.named_scope(f"i_wait{i}"):
            pending["g", i].wait_recv()
        total = acc[:, c] + precv[2 * i : 2 * i + 2].astype(f32)
        fsend[2 * i : 2 * i + 2] = total.astype(bf16)
        if i == last:
            yback[i, h] = fsend[2 * i + h]
            src = fsend.at[2 * i + 1 - h]
            begin(remote(src, yback.at[i, h], fy_s.at[0], fy_r.at[i, h], mate))
            return
        if i == far:
            half[...] = total
            copy = remote(fsend.at[2 * i + 1 - h], qrecv, qy_s.at[0], qy_r.at[0], mate)
            pending["i", i] = begin(copy)
            return
        for side in (0, 1):
            way = hops[i] + 1 if side else ys_n - hops[i]
            back = at(z, lax.rem(2 * pair + way, ys_n), c, x)
            k = 2 * i + side
            begin(remote(fsend.at[k], yback.at[i, h], fy_s.at[0], fy_r.at[i, h], back))

    def step_j(i):
        with jax.named_scope(f"j_wait{i}"):
            pending["i", i].wait_recv()
        fsend[2 * i + h] = (half[h] + qrecv[...].astype(f32)).astype(bf16)
        back = at(z, lax.rem(y + ys_n + hops[i] * (2 * h - 1), ys_n), c, x)
        k = 2 * i + h
        begin(remote(fsend.at[k], yback.at[i, 0], fy_s.at[0], fy_r.at[i, 0], back))

    def back_wait(i, hh):
        ref = yback.at[i, hh]
        remote(ref, ref, fy_s.at[0], fy_r.at[i, hh], mate).wait_recv()

    def zb_all(n):
        base = sum(g_rows[:n])
        ref = zgot.at[pl.ds(0, zs_n - 1), pl.ds(base, g_rows[n])]
        return remote(ref, ref, zb_s.at[n], zb_r.at[n], partner)

    def z_return(n):
        group, step = groups[n], g_rows[n]
        many = len(group) * erow
        perm = unpermutation(many, zs_n * step, step)
        with jax.named_scope(f"back_wait{n}"):
            for i in group:
                if i == last:
                    back_wait(i, 1 - h)
                elif i == far:
                    back_wait(i, 0)
                else:
                    back_wait(i, 0)
                    back_wait(i, 1)
        moved = 0.0
        for hh in (0,) if group == [far] else (0, 1):
            rows = yback[group[0] : group[-1] + 1, hh].reshape(many, dx)
            moved = moved + jnp.dot(perm, rows, preferred_element_type=f32)
        base = sum(g_rows[:n])
        zback[:, base : base + step] = moved.astype(bf16).reshape(zs_n, step, dx)
        rows = pl.ds(base, step)
        kept = []
        for r in near:
            zt = zpeer(r)
            copy = remote(
                zback.at[zt, rows], zgot.at[z, rows], zb_s.at[n], zb_r.at[n], at(zt, y, c, x)
            )
            copy.start()
            kept.append(copy)
        zgot[z, base : base + step] = zback[z, base : base + step]
        backs_z.extend(kept)
        returned.append((n, kept))

    def branch_core():
        with jax.named_scope("bz_wait"):
            bz_all().wait_recv()
        begin(remote(bw.at[:, :, :, c], bw.at[:, :, :, c], bc_s.at[0], bc_r.at[0], partner))

    def branch_dense():
        ref = bw.at[:, :, :, 1 - c]
        remote(ref, ref, bc_s.at[0], bc_r.at[0], partner).wait_recv()
        whole_in = bw[0].reshape(width, bw.shape[5])
        pre = jnp.dot(normed[...], whole_in, preferred_element_type=f32)
        hb = (pre / (1.0 + jnp.exp(-pre))).astype(bf16)
        for xx in range(xs_n):
            zpart = zs_n // xs_n if zs_n >= xs_n else 0
            if zpart:
                wo = bw[1, xx * zpart : (xx + 1) * zpart].reshape(dx, bw.shape[5])
            else:
                wo = bw[1].reshape(width, bw.shape[5])[xx * dx : (xx + 1) * dx]
            term = lax.dot_general(hb, wo, (((1,), (1,)), ((), ())), preferred_element_type=f32)
            bterm[xx] = term.astype(bf16)

    def branch_send():
        for r in range(1, xs_n):
            xt = xpeer(r)
            copy = remote(bterm.at[xt], bgot.at[r], bx_s.at[0], bx_r.at[0], at(z, y, c, xt))
            copy.start()
            bx.append(copy)

    order = ("d0", "d1", "n0", "m0", "d2", "n1", "m1", "n2", "b1", "m2", "planes", "b0", "c1", "b2", "e1", "c0", "c2", "o1", "e0", "f1", "e2", "g1", "f0", "o2", "f2", "e3", "i1", "g0", "core", "i0", "g2", "i2", "f3", "z0", "dense", "j2", "g3", "i3", "send", "z2", "z1")
    steps = dict(b=step_b, c=step_c, d=step_d, e=step_e, f=step_f, g=step_g, i=step_i, j=step_j)
    steps.update(m=step_m, n=step_n, o=step_o, z=z_return)
    others = dict(planes=branch_planes, core=branch_core, dense=branch_dense, send=branch_send)
    for item in order:
        if item in others:
            others[item]()
        else:
            steps[item[0]](int(item[1]))

    diff = scores_t[0:1, :] - scores_t[1:2, :]
    mixes = []
    for d in (diff, -diff):
        row = jnp.broadcast_to(sigmoid(d), sq)
        mixes.append(jnp.sum(jnp.where(sq_a == sq_b, row, 0.0), axis=1, keepdims=True))

    def combine(n):
        base = sum(g_rows[:n])
        shape = (zs_n * g_rows[n], rows_tok)
        t = lax.broadcasted_iota(jnp.int32, shape, 0).astype(f32) + 1.0 * g_low[n]
        rows = zgot[:, base : base + g_rows[n]].reshape(shape[0], dx)
        total = None
        for r in (0, 1):
            g = jnp.where(t == come[r], 1.0, 0.0).astype(bf16)
            term = lax.dot_general(g, rows, (((0,), (0,)), ((), ())), preferred_element_type=f32)
            total = mixes[r] * term if total is None else total + mixes[r] * term
        return total

    with jax.named_scope("bx_wait"):
        bx_all().wait_recv()
    share = bterm[x].astype(f32)
    for r in range(1, xs_n):
        share = share + bgot[r].astype(f32)
    share = share * branch_weight
    for n, kept in returned:
        with jax.named_scope(f"kept{n}"):
            if near:
                zb_all(n).wait_recv()
        share = share + combine(n)
    out[...] = share.astype(out.dtype)

    with jax.named_scope("send_wait"):
        if near:
            for i in range(1, pairs):
                zd_all(i).wait_send()
            for n in range(len(groups)):
                zb_all(n).wait_send()
            by_all().wait_send()
        bz_all().wait_send()
        bx_all().wait_send()
        narrow = 2 * last
        for ref, sem in (
            (tok.at[pl.ds(0, last), :, :, pl.ds(0, 3 * dx)], tx_s),
            (hid.at[:, :, :, pl.ds(0, 3 * fx)], hx_s),
            (tok.at[:, 0], tc_s),
            (tok.at[pl.ds(0, last + 2), :, :, pl.ds(0, dx)], yd_s),
            (fsend.at[pl.ds(0, narrow)], fy_s),
            (psend.at[:, 0], pc_s),
            (qrecv, qy_s),
            (bw.at[:, :, :, 0], bc_s),
        ):
            remote(ref, ref, sem.at[0], qy_r.at[0], partner).wait_send()


def on_device(
    cores_z,
    cores_y,
    tokens,
    norm_gain,
    routes,
    route_scores,
    expert_gate,
    expert_up,
    expert_down,
    branch_in,
    branch_out,
    branch_gate,
):
    zs_n, ys_n = cores_z, cores_y
    xs_n = lax.axis_size("tp")
    rows_tok, width = tokens.shape
    experts = zs_n * ys_n // 2
    cap = 5 * rows_tok * routes.shape[1] // (4 * experts)
    pairs = ys_n // 2
    dx = width // xs_n
    fx = expert_gate.shape[2]
    fg = expert_down.shape[1]
    arow = round_up(cap, 16)
    erow = round_up(zs_n * cap, 16)
    back_rows = sum(round_up(len(g) * cap, 16) for g in return_groups(pairs))
    bpart = branch_in.shape
    bf16, f32 = jnp.bfloat16, jnp.float32
    vm = lambda shape, dtype=bf16: pltpu.VMEM(shape, dtype)
    sem = lambda *shape: pltpu.SemaphoreType.DMA(shape)
    scratch = [
        vm((rows_tok, width)),
        vm((pairs - 1, zs_n, arow, dx)),
        vm((pairs - 1, zs_n, arow, dx)),
        vm((zs_n, arow, width)),
        vm((zs_n, arow, width)),
        vm((pairs - 1, erow, dx)),
        vm((ys_n, CORES, erow, width)),
        vm((width, 2 * fx)),
        vm((fg, dx)),
        vm((ys_n, CORES, erow, fg)),
        vm((2, CORES, erow, dx), f32),
        vm((ys_n, CORES, erow, dx)),
        vm((ys_n, erow, dx)),
        vm((2, erow, dx), f32),
        vm((erow, dx)),
        vm((ys_n, erow, dx)),
        vm((pairs, 2, erow, dx)),
        vm((zs_n, back_rows, dx)),
        vm((zs_n, back_rows, dx)),
        vm((2, zs_n, ys_n, CORES, *bpart)),
        vm((xs_n, rows_tok, dx)),
        vm((xs_n, rows_tok, dx)),
        sem(3),
        sem(pairs),
        sem(pairs),
        sem(1),
        sem(ys_n),
        sem(1),
        sem(3, ys_n),
        sem(1),
        sem(ys_n),
        sem(1),
        sem(3, ys_n),
        sem(1),
        sem(pairs),
        sem(1),
        sem(1),
        sem(1),
        sem(pairs, 2),
        sem(pairs),
        sem(pairs),
        sem(1),
        sem(1),
        sem(1),
        sem(1),
        sem(1),
        sem(1),
        sem(1),
        sem(1),
    ]
    in_vmem = pl.BlockSpec(memory_space=pltpu.VMEM)
    in_hbm = pl.BlockSpec(memory_space=pl.ANY)
    return pl.pallas_call(
        functools.partial(layer_kernel, zs_n, ys_n, xs_n, cap),
        out_shape=jax.ShapeDtypeStruct((rows_tok, dx), bf16),
        in_specs=[in_vmem] * 7 + [in_hbm] * 3,
        out_specs=in_vmem,
        scratch_shapes=scratch,
        compiler_params=pltpu.CompilerParams(
            collective_id=0, has_side_effects=True, vmem_limit_bytes=60 * 1024 * 1024
        ),
        name="routed_layer",
    )(
        tokens,
        norm_gain.reshape(1, -1),
        routes.T,
        route_scores.T,
        branch_gate.reshape(1, -1),
        branch_in,
        branch_out.T,
        expert_gate,
        expert_up,
        expert_down,
    )


def solution(mesh, z_y=None):
    ep = mesh.shape["ep"]
    zs_n, ys_n = z_y or (8, ep // (8 * CORES))
    in_specs = (
        P("ep", None),
        P(),
        P("ep", None),
        P("ep", None),
        P("ep", None, "tp"),
        P("ep", None, "tp"),
        P("ep", None, "tp"),
        P("ep", "tp"),
        P("tp", "ep"),
        P(),
    )
    return jax.shard_map(
        functools.partial(on_device, zs_n, ys_n),
        mesh=mesh,
        in_specs=in_specs,
        out_specs=P("ep", "tp"),
        check_vma=False,
    )
```

```python
import functools

import jax
import jax.numpy as jnp
from jax import lax
from jax.experimental import pallas as pl
from jax.experimental.pallas import tpu as pltpu
from jax.sharding import PartitionSpec as P

NORM_EPSILON = 1e-06
GROUP = 4
CORES = 2
MESH_ID = pl.DeviceIdType.MESH


def round_up(n, m):
    return (n + m - 1) // m * m


def sigmoid(v):
    return 1.0 / (1.0 + jnp.exp(-v))


def floor_div(v, n):
    return jnp.floor((v + 0.5) * (1.0 / n))


def return_groups(pairs):
    return [[0, 1], [2], [3]] if pairs == 4 else [[i] for i in range(pairs)]


def layer_kernel(
    zs_n,
    ys_n,
    xs_n,
    cap,
    tokens_h,
    gain_h,
    routes_h,
    scores_h,
    bgate_h,
    b_in_h,
    b_out_h,
    w_gate,
    w_up,
    w_down,
    out,
    tokens,
    gain,
    routes_t,
    scores_t,
    bgate,
    b_in,
    b_out,
    normed,
    zsend,
    zrecv,
    wsend,
    wrecv,
    ysend,
    tok,
    w_gu,
    w_dn,
    hid,
    acc,
    psend,
    precv,
    half,
    qrecv,
    fsend,
    yback,
    zback,
    zgot,
    bw,
    bterm,
    bgot,
    local_sem,
    zd_s,
    zd_r,
    yd_s,
    yd_r,
    tx_s,
    tx_r,
    tc_s,
    tc_r,
    hx_s,
    hx_r,
    pc_s,
    pc_r,
    qy_s,
    qy_r,
    fy_s,
    fy_r,
    zb_s,
    zb_r,
    by_s,
    by_r,
    bz_s,
    bz_r,
    bc_s,
    bc_r,
    bx_s,
    bx_r,
):
    f32, bf16 = jnp.float32, jnp.bfloat16
    ep = lax.axis_index("ep")
    x = lax.axis_index("tp")
    c = lax.rem(ep, CORES)
    y = lax.rem(ep // CORES, ys_n)
    z = ep // (CORES * ys_n)
    pairs = ys_n // 2
    pair = y // 2
    h = lax.rem(y, 2)
    hops = list(range(1, pairs)) + [0]
    last = pairs - 1
    offset = [last] + list(range(1, last)) + [0]
    rows_tok, width = tokens.shape
    dx = width // xs_n
    fx = w_gate.shape[2]
    groups = return_groups(pairs)
    lanes = 128
    parts = dx // lanes
    g_rows = [round_up(parts * len(g) * cap, 16) for g in groups]
    g_low = [zs_n * sum(g_rows[:n]) for n in range(len(groups))]
    experts = zs_n * pairs
    arow = zsend.shape[2]
    slots = zs_n * arow
    erow = ysend.shape[1]
    far = hops.index(last)

    def at(z_, y_, c_, x_):
        return ((z_ * ys_n + y_) * CORES + c_, x_)

    def zpeer(r):
        return lax.rem(z + r, zs_n)

    def ypeer(r):
        return lax.rem(y + r, ys_n)

    def xpeer(r):
        return lax.rem(x + r, xs_n)

    def remote(src, dst, s, r, dev):
        return pltpu.make_async_remote_copy(
            src_ref=src, dst_ref=dst, send_sem=s, recv_sem=r, device_id=dev, device_id_type=MESH_ID
        )

    barrier = pltpu.get_barrier_semaphore()
    peers = [at(zpeer(r), y, c, x) for r in range(1, zs_n)]
    peers += [at(z, ypeer(r), c, x) for r in range(1, ys_n)]
    peers += [at(z, y, c, xpeer(r)) for r in range(1, xs_n)]
    peers += [at(z, y, 1 - c, x)]
    for dev in peers:
        pl.semaphore_signal(barrier, inc=1, device_id=dev, device_id_type=MESH_ID)

    pairs_in = (
        (tokens_h, tokens),
        (routes_h, routes_t),
        (gain_h, gain),
        (b_in_h, b_in),
        (b_out_h, b_out),
        (bgate_h, bgate),
        (scores_h, scores_t),
    )
    fetched = [
        pltpu.make_async_copy(src, dst, local_sem.at[3 + n])
        for n, (src, dst) in enumerate(pairs_in)
    ]
    for copy in fetched:
        copy.start()
    weights = [
        pltpu.make_async_copy(w_gate.at[0], w_gu.at[:, pl.ds(0, fx)], local_sem.at[0]),
        pltpu.make_async_copy(w_up.at[0], w_gu.at[:, pl.ds(fx, fx)], local_sem.at[1]),
        pltpu.make_async_copy(w_down.at[0], w_dn, local_sem.at[2]),
    ]
    for copy in weights:
        copy.start()

    for copy in fetched:
        copy.wait()
    tf = tokens[...].astype(f32)
    scaled = lax.rsqrt(jnp.sum(tf * tf, axis=-1, keepdims=True) * (1.0 / width) + NORM_EPSILON)
    nf = (tf * scaled * gain[...]).astype(bf16)
    normed[...] = nf

    ids = lax.broadcasted_iota(jnp.int32, (experts, rows_tok), 0)
    sq = (rows_tok, rows_tok)
    sq_a = lax.broadcasted_iota(jnp.int32, sq, 0)
    sq_b = lax.broadcasted_iota(jnp.int32, sq, 1)
    chosen = [jnp.where(ids == routes_t[r : r + 1, :], 1.0, 0.0) for r in (0, 1)]
    earlier = jnp.where(sq_a < sq_b, 1.0, 0.0).astype(bf16)
    ranks = jnp.dot((chosen[0] + chosen[1]).astype(bf16), earlier, preferred_element_type=f32)
    go, come = [], []
    for r in (0, 1):
        rank = jnp.sum(chosen[r] * ranks, axis=0, keepdims=True)
        e = routes_t[r : r + 1, :].astype(f32)
        zz = floor_div(e, pairs)
        v = (e - zz * pairs - pair.astype(f32)) * (1 - 2 * h).astype(f32) + pairs
        rel = jnp.where(v >= pairs, v - pairs, v)
        rel = jnp.where(rel < 0.5, 1.0 * last, jnp.where(rel > last - 0.5, 0.0, rel))
        go.append(rank + rel * slots + zz * arow)
        place = 0.0
        for group, n_rows, low in zip(groups, g_rows, g_low):
            spot = low + zz * n_rows + (rel - group[0]) * cap
            place = spot if group[0] == 0 else jnp.where(rel > group[0] - 0.5, spot, place)
        come.append(rank + place)
    srow = lax.broadcasted_iota(jnp.int32, (pairs * slots, rows_tok), 0).astype(f32)
    pick = jnp.where((srow == go[0]) | (srow == go[1]), 1.0, 0.0).astype(bf16)
    own_cols = pl.ds(pl.multiple_of(x * dx, dx), dx)
    packed = jnp.dot(pick[: last * slots], normed[:, own_cols], preferred_element_type=f32)
    zsend[...] = packed.astype(bf16).reshape(last, zs_n, arow, dx)

    pl.semaphore_wait(barrier, len(peers))

    zd, by = {}, []
    near = sorted(range(1, zs_n), key=lambda r: min(r, zs_n - r))

    def z_send(i):
        src, dst = (wsend, wrecv) if i == last else (zsend.at[i], zrecv.at[i])
        zd[i] = []
        for r in near:
            zt = zpeer(r)
            copy = remote(src.at[zt], dst.at[z], zd_s.at[i], zd_r.at[i], at(zt, y, c, x))
            copy.start()
            zd[i].append(copy)

    def zd_all(i):
        ref = wrecv if i == last else zrecv.at[i]
        ref = ref.at[pl.ds(0, zs_n - 1)]
        return remote(ref, ref, zd_s.at[i], zd_r.at[i], at(z, y, 1 - c, x))

    z_send(0)
    for i in range(last):
        zrecv[i, z] = zsend[i, z]
    wide = jnp.dot(pick[last * slots :], normed[...], preferred_element_type=f32)
    wsend[...] = wide.astype(bf16).reshape(zs_n, arow, width)
    wrecv[z] = wsend[z]
    if near:
        zd_all(0).wait_send()
    z_send(1)
    for r in near:
        for w, part in enumerate((b_in, b_out)):
            copy = remote(
                part, bw.at[w, z, y, c], by_s.at[0], by_r.at[0], at(zpeer(r), y, c, x)
            )
            copy.start()
            by.append(copy)
    bw[0, z, y, c] = b_in[...]
    bw[1, z, y, c] = b_out[...]

    bsum = jnp.sum(normed[...].astype(f32) * bgate[...], axis=-1, keepdims=True)
    branch_weight = sigmoid(bsum)

    def row_target(q, step):
        pp = floor_div(q, erow)
        rem = q - pp * erow
        zz = floor_div(rem, cap)
        return jnp.where(zz < zs_n, zz * step + pp * cap + (rem - zz * cap), -1e6)

    def permutation(rows, slots, step):
        q = lax.broadcasted_iota(jnp.int32, (rows, slots), 0).astype(f32)
        t = lax.broadcasted_iota(jnp.int32, (rows, slots), 1).astype(f32)
        return jnp.where(row_target(q, step) == t, 1.0, 0.0).astype(bf16)

    def unpermutation(rows, slots, step, shift):
        q = lax.broadcasted_iota(jnp.int32, (slots, rows), 1).astype(f32)
        t = lax.broadcasted_iota(jnp.int32, (slots, rows), 0).astype(f32)
        return jnp.where(row_target(q, step) + shift == t, 1.0, 0.0).astype(bf16)

    east, west = at(z, y, c, xpeer(1)), at(z, y, c, xpeer(xs_n - 1))
    partner = at(z, y, 1 - c, x)
    mate = at(z, y + 1 - 2 * h, c, x)
    started, bz, bx, backs_z, returned = [], [], [], [], []
    pending = {}

    def begin(copy):
        copy.start()
        started.append(copy)
        return copy

    def tok_part(k, xx):
        return tok.at[k, c, :, pl.ds(pl.multiple_of(xx * dx, dx), dx)]

    def hid_part(k, xx):
        return hid.at[k, :, :, pl.ds(pl.multiple_of(xx * fx, fx), fx)]

    def spread(part, sems, rsems, k):
        for way, dev in ((0, east), (1, west)):
            begin(remote(part(k, x), part(k, x), sems.at[0], rsems.at[way, k], dev))

    def arrive(part, rsems, sems, way, k):
        ref = part(k, x)
        remote(ref, ref, sems.at[0], rsems.at[way, k], east).wait_recv()

    def relay(part, sems, rsems, k):
        way = lax.rem(k, 2)
        arrive(part, rsems, sems, way, k)
        ref = part(k, xpeer(xs_n - 1 - 2 * way))
        dev = at(z, y, c, xpeer(1 + 2 * way))
        begin(remote(ref, ref, sems.at[0], rsems.at[2, k], dev))

    def settle(part, sems, rsems, k):
        arrive(part, rsems, sems, 1 - k % 2, k)
        arrive(part, rsems, sems, 2, k)

    def y_wait(k):
        ref = tok.at[k, c, :, own_cols]
        remote(ref, ref, yd_s.at[0], yd_r.at[k], mate).wait_recv()

    def both(i):
        return (2 * i, 2 * i + 1)

    def step_d(i):
        perm = permutation(erow, slots, arow)
        with jax.named_scope(f"z_wait{i}"):
            if near:
                zd_all(i).wait_recv()
        moved = jnp.dot(perm, zrecv[i].reshape(slots, dx), preferred_element_type=f32)
        ysend[i] = moved.astype(bf16)
        pt = lax.rem(pair + pairs + offset[i] * (1 - 2 * h), pairs)
        near_chip = lax.rem(h + hops[i], 2)
        k = 2 * i + near_chip
        for n, hh in enumerate((near_chip, 1 - near_chip)):
            if i == far and n == 1:
                break
            dst = tok.at[k, c, :, own_cols]
            dev = at(z, 2 * pt + hh, c, x)
            begin(remote(ysend.at[i], dst, yd_s.at[0], yd_r.at[k], dev))
        if i + 2 <= last:
            z_send(i + 2)

    def to_partner(k, ref):
        begin(remote(ref, ref, tc_s.at[0], tc_r.at[k], partner))

    def step_o(part):
        mine = 2 * last + h
        if part == 1:
            perm = permutation(erow, slots, arow)
            with jax.named_scope("z_wait_wide"):
                if near:
                    zd_all(last).wait_recv()
            moved = jnp.dot(perm, wrecv[...].reshape(slots, width), preferred_element_type=f32)
            tok[mine, c] = moved.astype(bf16)
            ref = tok.at[mine, c]
            begin(remote(ref, ref, yd_s.at[0], yd_r.at[mine], mate))
            to_partner(mine, ref)
            return
        ref = tok.at[2 * last + 1 - h, c]
        with jax.named_scope("wide_mate"):
            remote(ref, ref, yd_s.at[0], yd_r.at[2 * last + 1 - h], mate).wait_recv()
        to_partner(2 * last + 1 - h, ref)

    def by_all():
        ref = bw.at[:, 0, pl.ds(0, zs_n - 1), 0]
        return remote(ref, ref, by_s.at[0], by_r.at[0], partner)

    def bz_all():
        ref = bw.at[:, :, pl.ds(0, ys_n - 1), 0]
        return remote(ref, ref, bz_s.at[0], bz_r.at[0], partner)

    def bx_all():
        ref = bgot.at[pl.ds(0, xs_n - 1)]
        return remote(ref, ref, bx_s.at[0], bx_r.at[0], partner)

    def branch_planes():
        if near:
            by_all().wait_recv()
        for r in range(1, ys_n):
            part = bw.at[:, :, y, c]
            copy = remote(part, part, bz_s.at[0], bz_r.at[0], at(z, ypeer(r), c, x))
            copy.start()
            bz.append(copy)

    def step_n(i):
        mine = 2 * i + h
        with jax.named_scope(f"n_wait{i}"):
            y_wait(mine)
        if i == far:
            ref = tok.at[mine, c, :, own_cols]
            begin(remote(ref, ref, yd_s.at[0], yd_r.at[mine], mate))
        spread(tok_part, tx_s, tx_r, mine)
        to_partner(mine, tok_part(mine, x))

    def step_m(i):
        with jax.named_scope(f"m_wait{i}"):
            y_wait(2 * i + 1 - h)
        k = 2 * i + 1 - h
        spread(tok_part, tx_s, tx_r, k)
        to_partner(k, tok_part(k, x))

    def step_b(i):
        for n, k in enumerate((2 * i + h, 2 * i + 1 - h)):
            with jax.named_scope(f"b_relay{i}_{n}"):
                relay(tok_part, tx_s, tx_r, k)
            to_partner(k, tok_part(k, xpeer(xs_n - 1 - 2 * lax.rem(k, 2))))

    def step_c(i):
        for k in both(i):
            way = k % 2
            with jax.named_scope(f"c_settle{k}"):
                arrive(tok_part, tx_r, tx_s, 1 - way, k)
            to_partner(k, tok_part(k, xpeer(1 + 2 * way)))
        for k in both(i):
            with jax.named_scope(f"c_last{k}"):
                arrive(tok_part, tx_r, tx_s, 2, k)
            to_partner(k, tok_part(k, xpeer(2)))

    def step_e(i):
        with jax.named_scope(f"e_wait{i}"):
            for k in both(i):
                ref = tok.at[k, 1 - c]
                remote(ref, ref, tc_s.at[0], tc_r.at[k], partner).wait_recv()
            while len(weights) > 1:
                weights.pop(0).wait()
        with jax.named_scope(f"e_dot{i}"):
            rows = tok[2 * i : 2 * i + 2].reshape(2 * CORES * erow, width)
            pre = jnp.dot(rows, w_gu[...], preferred_element_type=f32)
            gate, up = pre[:, :fx], pre[:, fx:]
            hidden = (gate / (1.0 + jnp.exp(-gate)) * up).astype(bf16)
            cols = pl.ds(pl.multiple_of(x * fx, fx), fx)
            hid[2 * i : 2 * i + 2, :, :, cols] = hidden.reshape(2, CORES, erow, fx)
        for k in both(i):
            spread(hid_part, hx_s, hx_r, k)

    def step_f(i):
        for k in both(i):
            with jax.named_scope(f"f_relay{k}"):
                relay(hid_part, hx_s, hx_r, k)

    def step_g(i):
        for k in both(i):
            with jax.named_scope(f"g_settle{k}"):
                settle(hid_part, hx_s, hx_r, k)
        while weights:
            weights.pop(0).wait()
        with jax.named_scope(f"g_dot{i}"):
            rows = hid[2 * i : 2 * i + 2].reshape(2 * CORES * erow, hid.shape[3])
            part = jnp.dot(rows, w_dn[...], preferred_element_type=f32)
            part = part.reshape(2, CORES, erow, dx)
            acc[...] = part
            psend[2 * i : 2 * i + 2] = part.astype(bf16)
        two = pl.ds(2 * i, 2)
        pending["g", i] = begin(
            remote(psend.at[two, 1 - c], precv.at[two], pc_s.at[0], pc_r.at[i], partner)
        )

    def step_i(i):
        with jax.named_scope(f"i_wait{i}"):
            pending["g", i].wait_recv()
        total = acc[:, c] + precv[2 * i : 2 * i + 2].astype(f32)
        fsend[2 * i : 2 * i + 2] = total.astype(bf16)
        if i == last:
            yback[i, h] = fsend[2 * i + h]
            src = fsend.at[2 * i + 1 - h]
            begin(remote(src, yback.at[i, h], fy_s.at[0], fy_r.at[i, h], mate))
            return
        if i == far:
            half[...] = total
            copy = remote(fsend.at[2 * i + 1 - h], qrecv, qy_s.at[0], qy_r.at[0], mate)
            pending["i", i] = begin(copy)
            return
        for side in (0, 1):
            way = hops[i] + 1 if side else ys_n - hops[i]
            back = at(z, lax.rem(2 * pair + way, ys_n), c, x)
            k = 2 * i + side
            begin(remote(fsend.at[k], yback.at[i, h], fy_s.at[0], fy_r.at[i, h], back))

    def step_j(i):
        with jax.named_scope(f"j_wait{i}"):
            pending["i", i].wait_recv()
        fsend[2 * i + h] = (half[h] + qrecv[...].astype(f32)).astype(bf16)
        back = at(z, lax.rem(y + ys_n + hops[i] * (2 * h - 1), ys_n), c, x)
        k = 2 * i + h
        begin(remote(fsend.at[k], yback.at[i, 0], fy_s.at[0], fy_r.at[i, 0], back))

    def back_wait(i, hh):
        ref = yback.at[i, hh]
        remote(ref, ref, fy_s.at[0], fy_r.at[i, hh], mate).wait_recv()

    def zb_all(n):
        base = sum(g_rows[:n])
        ref = zgot.at[pl.ds(0, zs_n - 1), pl.ds(base, g_rows[n])]
        return remote(ref, ref, zb_s.at[n], zb_r.at[n], partner)

    def z_return(n):
        group, step = groups[n], g_rows[n]
        many = len(group) * erow
        perms = [
            unpermutation(many, zs_n * step, step, 1.0 * cc * len(group) * cap)
            for cc in range(parts)
        ]
        with jax.named_scope(f"back_wait{n}"):
            for i in group:
                if i == last:
                    back_wait(i, 1 - h)
                elif i == far:
                    back_wait(i, 0)
                else:
                    back_wait(i, 0)
                    back_wait(i, 1)
        moved = 0.0
        for hh in (0,) if group == [far] else (0, 1):
            rows = yback[group[0] : group[-1] + 1, hh].reshape(many, dx)
            for cc, perm in enumerate(perms):
                piece = rows[:, cc * lanes : (cc + 1) * lanes]
                moved = moved + jnp.dot(perm, piece, preferred_element_type=f32)
        base = sum(g_rows[:n])
        zback[:, base : base + step] = moved.astype(bf16).reshape(zs_n, step, lanes)
        rows = pl.ds(base, step)
        kept = []
        for r in near:
            zt = zpeer(r)
            copy = remote(
                zback.at[zt, rows], zgot.at[z, rows], zb_s.at[n], zb_r.at[n], at(zt, y, c, x)
            )
            copy.start()
            kept.append(copy)
        zgot[z, base : base + step] = zback[z, base : base + step]
        backs_z.extend(kept)
        returned.append((n, kept))

    def branch_core():
        with jax.named_scope("bz_wait"):
            bz_all().wait_recv()
        begin(remote(bw.at[:, :, :, c], bw.at[:, :, :, c], bc_s.at[0], bc_r.at[0], partner))

    def branch_dense():
        ref = bw.at[:, :, :, 1 - c]
        remote(ref, ref, bc_s.at[0], bc_r.at[0], partner).wait_recv()
        whole_in = bw[0].reshape(width, bw.shape[5])
        pre = jnp.dot(normed[...], whole_in, preferred_element_type=f32)
        hb = (pre / (1.0 + jnp.exp(-pre))).astype(bf16)
        for xx in range(xs_n):
            zpart = zs_n // xs_n if zs_n >= xs_n else 0
            if zpart:
                wo = bw[1, xx * zpart : (xx + 1) * zpart].reshape(dx, bw.shape[5])
            else:
                wo = bw[1].reshape(width, bw.shape[5])[xx * dx : (xx + 1) * dx]
            term = lax.dot_general(hb, wo, (((1,), (1,)), ((), ())), preferred_element_type=f32)
            bterm[xx] = term.astype(bf16)

    def branch_send():
        for r in range(1, xs_n):
            xt = xpeer(r)
            copy = remote(bterm.at[xt], bgot.at[r], bx_s.at[0], bx_r.at[0], at(z, y, c, xt))
            copy.start()
            bx.append(copy)

    order = ("d0", "d1", "n0", "m0", "d2", "n1", "m1", "n2", "b1", "m2", "planes", "b0", "c1", "b2", "e1", "c0", "c2", "o1", "e0", "f1", "e2", "g1", "f0", "o2", "f2", "e3", "i1", "g0", "core", "i0", "g2", "i2", "f3", "dense", "j2", "g3", "z0", "i3", "send", "z2", "z1")
    steps = dict(b=step_b, c=step_c, d=step_d, e=step_e, f=step_f, g=step_g, i=step_i, j=step_j)
    steps.update(m=step_m, n=step_n, o=step_o, z=z_return)
    others = dict(planes=branch_planes, core=branch_core, dense=branch_dense, send=branch_send)
    for item in order:
        if item in others:
            others[item]()
        else:
            steps[item[0]](int(item[1]))

    diff = scores_t[0:1, :] - scores_t[1:2, :]
    mixes = []
    for d in (diff, -diff):
        row = jnp.broadcast_to(sigmoid(d), sq)
        mixes.append(jnp.sum(jnp.where(sq_a == sq_b, row, 0.0), axis=1, keepdims=True))

    def column(row):
        wide_row = jnp.broadcast_to(row, sq)
        return jnp.sum(jnp.where(sq_a == sq_b, wide_row, 0.0), axis=1, keepdims=True)

    spots = [column(come[r]) for r in (0, 1)]

    def picks(n):
        shape = (rows_tok, zs_n * g_rows[n])
        t = lax.broadcasted_iota(jnp.int32, shape, 1).astype(f32) + 1.0 * g_low[n]
        size = len(groups[n]) * cap
        return [
            [jnp.where(t == spots[r] + 1.0 * cc * size, 1.0, 0.0).astype(bf16) for cc in range(parts)]
            for r in (0, 1)
        ]

    def combine(n, taken):
        base = sum(g_rows[:n])
        rows = zgot[:, base : base + g_rows[n]].reshape(zs_n * g_rows[n], lanes)
        terms = []
        for cc in range(parts):
            one = jnp.dot(taken[0][cc], rows, preferred_element_type=f32)
            two = jnp.dot(taken[1][cc], rows, preferred_element_type=f32)
            terms.append(mixes[0] * one + mixes[1] * two)
        return jnp.concatenate(terms, axis=1)

    with jax.named_scope("bx_wait"):
        bx_all().wait_recv()
    share = bterm[x].astype(f32)
    for r in range(1, xs_n):
        share = share + bgot[r].astype(f32)
    share = share * branch_weight
    for n, _ in returned:
        taken = picks(n)
        with jax.named_scope(f"kept{n}"):
            if near:
                zb_all(n).wait_recv()
        share = share + combine(n, taken)
    out[...] = share.astype(out.dtype)

    with jax.named_scope("send_wait"):
        if near:
            for i in range(1, pairs):
                zd_all(i).wait_send()
            for n in range(len(groups)):
                zb_all(n).wait_send()
            by_all().wait_send()
        bz_all().wait_send()
        bx_all().wait_send()
        narrow = 2 * last
        for ref, sem in (
            (tok.at[pl.ds(0, last), :, :, pl.ds(0, 3 * dx)], tx_s),
            (hid.at[:, :, :, pl.ds(0, 3 * fx)], hx_s),
            (tok.at[:, 0], tc_s),
            (tok.at[pl.ds(0, last + 2), :, :, pl.ds(0, dx)], yd_s),
            (fsend.at[pl.ds(0, narrow)], fy_s),
            (psend.at[:, 0], pc_s),
            (qrecv, qy_s),
            (bw.at[:, :, :, 0], bc_s),
        ):
            remote(ref, ref, sem.at[0], qy_r.at[0], partner).wait_send()


def on_device(
    cores_z,
    cores_y,
    tokens,
    norm_gain,
    routes,
    route_scores,
    expert_gate,
    expert_up,
    expert_down,
    branch_in,
    branch_out,
    branch_gate,
):
    zs_n, ys_n = cores_z, cores_y
    xs_n = lax.axis_size("tp")
    rows_tok, width = tokens.shape
    experts = zs_n * ys_n // 2
    cap = 5 * rows_tok * routes.shape[1] // (4 * experts)
    pairs = ys_n // 2
    dx = width // xs_n
    fx = expert_gate.shape[2]
    fg = expert_down.shape[1]
    arow = round_up(cap, 16)
    erow = round_up(zs_n * cap, 16)
    back_rows = sum(round_up(dx // 128 * len(g) * cap, 16) for g in return_groups(pairs))
    bpart = branch_in.shape
    bf16, f32 = jnp.bfloat16, jnp.float32
    vm = lambda shape, dtype=bf16: pltpu.VMEM(shape, dtype)
    sem = lambda *shape: pltpu.SemaphoreType.DMA(shape)
    scratch = [
        vm((rows_tok, width)),
        vm((1, width), f32),
        vm((2, rows_tok), jnp.int32),
        vm((2, rows_tok), f32),
        vm((1, width), f32),
        vm(bpart),
        vm(bpart),
        vm((rows_tok, width)),
        vm((pairs - 1, zs_n, arow, dx)),
        vm((pairs - 1, zs_n, arow, dx)),
        vm((zs_n, arow, width)),
        vm((zs_n, arow, width)),
        vm((pairs - 1, erow, dx)),
        vm((ys_n, CORES, erow, width)),
        vm((width, 2 * fx)),
        vm((fg, dx)),
        vm((ys_n, CORES, erow, fg)),
        vm((2, CORES, erow, dx), f32),
        vm((ys_n, CORES, erow, dx)),
        vm((ys_n, erow, dx)),
        vm((2, erow, dx), f32),
        vm((erow, dx)),
        vm((ys_n, erow, dx)),
        vm((pairs, 2, erow, dx)),
        vm((zs_n, back_rows, 128)),
        vm((zs_n, back_rows, 128)),
        vm((2, zs_n, ys_n, CORES, *bpart)),
        vm((xs_n, rows_tok, dx)),
        vm((xs_n, rows_tok, dx)),
        sem(10),
        sem(pairs),
        sem(pairs),
        sem(1),
        sem(ys_n),
        sem(1),
        sem(3, ys_n),
        sem(1),
        sem(ys_n),
        sem(1),
        sem(3, ys_n),
        sem(1),
        sem(pairs),
        sem(1),
        sem(1),
        sem(1),
        sem(pairs, 2),
        sem(pairs),
        sem(pairs),
        sem(1),
        sem(1),
        sem(1),
        sem(1),
        sem(1),
        sem(1),
        sem(1),
        sem(1),
    ]
    in_vmem = pl.BlockSpec(memory_space=pltpu.VMEM)
    in_hbm = pl.BlockSpec(memory_space=pl.ANY)
    return pl.pallas_call(
        functools.partial(layer_kernel, zs_n, ys_n, xs_n, cap),
        out_shape=jax.ShapeDtypeStruct((rows_tok, dx), bf16),
        in_specs=[in_hbm] * 10,
        out_specs=in_vmem,
        scratch_shapes=scratch,
        compiler_params=pltpu.CompilerParams(
            collective_id=0, has_side_effects=True, vmem_limit_bytes=60 * 1024 * 1024
        ),
        name="routed_layer",
    )(
        tokens,
        norm_gain.reshape(1, -1),
        routes.T,
        route_scores.T,
        branch_gate.reshape(1, -1),
        branch_in,
        branch_out.T,
        expert_gate,
        expert_up,
        expert_down,
    )


def solution(mesh, z_y=None):
    ep = mesh.shape["ep"]
    zs_n, ys_n = z_y or (8, ep // (8 * CORES))
    in_specs = (
        P("ep", None),
        P(),
        P("ep", None),
        P("ep", None),
        P("ep", None, "tp"),
        P("ep", None, "tp"),
        P("ep", None, "tp"),
        P("ep", "tp"),
        P("tp", "ep"),
        P(),
    )
    return jax.shard_map(
        functools.partial(on_device, zs_n, ys_n),
        mesh=mesh,
        in_specs=in_specs,
        out_specs=P("ep", "tp"),
        check_vma=False,
    )
```

```python
import functools

import jax
import jax.numpy as jnp
from jax import lax
from jax.experimental import pallas as pl
from jax.experimental.pallas import tpu as pltpu
from jax.sharding import PartitionSpec as P

NORM_EPSILON = 1e-06
GROUP = 4
CORES = 2
MESH_ID = pl.DeviceIdType.MESH


def round_up(n, m):
    return (n + m - 1) // m * m


def sigmoid(v):
    return 1.0 / (1.0 + jnp.exp(-v))


def floor_div(v, n):
    return jnp.floor((v + 0.5) * (1.0 / n))


def return_groups(pairs):
    return [[0, 1], [2], [3]] if pairs == 4 else [[i] for i in range(pairs)]


def layer_kernel(
    zs_n,
    ys_n,
    xs_n,
    cap,
    tokens_h,
    gain_h,
    routes_h,
    scores_h,
    bgate_h,
    b_in_h,
    b_out_h,
    w_gate,
    w_up,
    w_down,
    out,
    tokens,
    gain,
    routes_t,
    scores_t,
    bgate,
    b_in,
    b_out,
    normed,
    zsend,
    zrecv,
    wsend,
    wrecv,
    ysend,
    tok,
    w_gu,
    w_dn,
    hid,
    acc,
    psend,
    precv,
    perms,
    half,
    qrecv,
    fsend,
    yback,
    zback,
    zgot,
    bw,
    bterm,
    bgot,
    local_sem,
    zd_s,
    zd_r,
    yd_s,
    yd_r,
    tx_s,
    tx_r,
    tc_s,
    tc_r,
    hx_s,
    hx_r,
    pc_s,
    pc_r,
    qy_s,
    qy_r,
    fy_s,
    fy_r,
    zb_s,
    zb_r,
    by_s,
    by_r,
    bz_s,
    bz_r,
    bc_s,
    bc_r,
    bx_s,
    bx_r,
):
    f32, bf16 = jnp.float32, jnp.bfloat16
    ep = lax.axis_index("ep")
    x = lax.axis_index("tp")
    c = lax.rem(ep, CORES)
    y = lax.rem(ep // CORES, ys_n)
    z = ep // (CORES * ys_n)
    pairs = ys_n // 2
    pair = y // 2
    h = lax.rem(y, 2)
    hops = list(range(1, pairs)) + [0]
    last = pairs - 1
    offset = [last] + list(range(1, last)) + [0]
    rows_tok, width = tokens.shape
    dx = width // xs_n
    fx = w_gate.shape[2]
    groups = return_groups(pairs)
    lanes = 128
    parts = dx // lanes
    g_rows = [round_up(parts * len(g) * cap, 16) for g in groups]
    g_low = [zs_n * sum(g_rows[:n]) for n in range(len(groups))]
    experts = zs_n * pairs
    arow = zsend.shape[2]
    slots = zs_n * arow
    erow = ysend.shape[1]
    far = hops.index(last)

    def at(z_, y_, c_, x_):
        return ((z_ * ys_n + y_) * CORES + c_, x_)

    def zpeer(r):
        return lax.rem(z + r, zs_n)

    def ypeer(r):
        return lax.rem(y + r, ys_n)

    def xpeer(r):
        return lax.rem(x + r, xs_n)

    def remote(src, dst, s, r, dev):
        return pltpu.make_async_remote_copy(
            src_ref=src, dst_ref=dst, send_sem=s, recv_sem=r, device_id=dev, device_id_type=MESH_ID
        )

    barrier = pltpu.get_barrier_semaphore()
    peers = [at(zpeer(r), y, c, x) for r in range(1, zs_n)]
    peers += [at(z, ypeer(r), c, x) for r in range(1, ys_n)]
    peers += [at(z, y, c, xpeer(r)) for r in range(1, xs_n)]
    peers += [at(z, y, 1 - c, x)]
    for dev in peers:
        pl.semaphore_signal(barrier, inc=1, device_id=dev, device_id_type=MESH_ID)

    pairs_in = (
        (tokens_h, tokens),
        (routes_h, routes_t),
        (gain_h, gain),
        (b_in_h, b_in),
        (b_out_h, b_out),
        (bgate_h, bgate),
        (scores_h, scores_t),
    )
    fetched = [
        pltpu.make_async_copy(src, dst, local_sem.at[3 + n])
        for n, (src, dst) in enumerate(pairs_in)
    ]
    for copy in fetched:
        copy.start()
    weights = [
        pltpu.make_async_copy(w_gate.at[0], w_gu.at[:, pl.ds(0, fx)], local_sem.at[0]),
        pltpu.make_async_copy(w_up.at[0], w_gu.at[:, pl.ds(fx, fx)], local_sem.at[1]),
        pltpu.make_async_copy(w_down.at[0], w_dn, local_sem.at[2]),
    ]
    for copy in weights:
        copy.start()

    for copy in fetched:
        copy.wait()
    tf = tokens[...].astype(f32)
    scaled = lax.rsqrt(jnp.sum(tf * tf, axis=-1, keepdims=True) * (1.0 / width) + NORM_EPSILON)
    nf = (tf * scaled * gain[...]).astype(bf16)
    normed[...] = nf

    ids = lax.broadcasted_iota(jnp.int32, (experts, rows_tok), 0)
    sq = (rows_tok, rows_tok)
    sq_a = lax.broadcasted_iota(jnp.int32, sq, 0)
    sq_b = lax.broadcasted_iota(jnp.int32, sq, 1)
    chosen = [jnp.where(ids == routes_t[r : r + 1, :], 1.0, 0.0) for r in (0, 1)]
    earlier = jnp.where(sq_a < sq_b, 1.0, 0.0).astype(bf16)
    ranks = jnp.dot((chosen[0] + chosen[1]).astype(bf16), earlier, preferred_element_type=f32)
    go, come = [], []
    for r in (0, 1):
        rank = jnp.sum(chosen[r] * ranks, axis=0, keepdims=True)
        e = routes_t[r : r + 1, :].astype(f32)
        zz = floor_div(e, pairs)
        v = (e - zz * pairs - pair.astype(f32)) * (1 - 2 * h).astype(f32) + pairs
        rel = jnp.where(v >= pairs, v - pairs, v)
        rel = jnp.where(rel < 0.5, 1.0 * last, jnp.where(rel > last - 0.5, 0.0, rel))
        go.append(rank + rel * slots + zz * arow)
        place = 0.0
        for group, n_rows, low in zip(groups, g_rows, g_low):
            spot = low + zz * n_rows + (rel - group[0]) * cap
            place = spot if group[0] == 0 else jnp.where(rel > group[0] - 0.5, spot, place)
        come.append(rank + place)
    own_cols = pl.ds(pl.multiple_of(x * dx, dx), dx)
    wide_lanes = width // parts

    def pack(i, source, n_lanes):
        srow = lax.broadcasted_iota(jnp.int32, (slots, rows_tok), 0).astype(f32) + 1.0 * i * slots
        total = 0.0
        for cc in range(parts):
            here = srow - 1.0 * cc * cap
            pick = jnp.where((here == go[0]) | (here == go[1]), 1.0, 0.0).astype(bf16)
            total = total + jnp.dot(pick, source(cc), preferred_element_type=f32)
        return total.astype(bf16).reshape(zs_n, arow, n_lanes)

    def narrow_source(cc):
        start = pl.multiple_of(x * dx + cc * lanes, lanes)
        return normed[:, pl.ds(start, lanes)]

    def wide_source(cc):
        return normed[:, cc * wide_lanes : (cc + 1) * wide_lanes]

    zsend[0] = pack(0, narrow_source, lanes)

    pl.semaphore_wait(barrier, len(peers))

    zd, by = {}, []
    near = sorted(range(1, zs_n), key=lambda r: min(r, zs_n - r))

    def z_send(i):
        src, dst = (wsend, wrecv) if i == last else (zsend.at[i], zrecv.at[i])
        zd[i] = []
        for r in near:
            zt = zpeer(r)
            copy = remote(src.at[zt], dst.at[z], zd_s.at[i], zd_r.at[i], at(zt, y, c, x))
            copy.start()
            zd[i].append(copy)

    def zd_all(i):
        ref = wrecv if i == last else zrecv.at[i]
        ref = ref.at[pl.ds(0, zs_n - 1)]
        return remote(ref, ref, zd_s.at[i], zd_r.at[i], at(z, y, 1 - c, x))

    z_send(0)
    for i in range(1, last):
        zsend[i] = pack(i, narrow_source, lanes)
    for i in range(last):
        zrecv[i, z] = zsend[i, z]
    if near:
        zd_all(0).wait_send()
    z_send(1)
    for r in near:
        for w, part in enumerate((b_in, b_out)):
            copy = remote(
                part, bw.at[w, z, y, c], by_s.at[0], by_r.at[0], at(zpeer(r), y, c, x)
            )
            copy.start()
            by.append(copy)
    bw[0, z, y, c] = b_in[...]
    bw[1, z, y, c] = b_out[...]

    bsum = jnp.sum(normed[...].astype(f32) * bgate[...], axis=-1, keepdims=True)
    branch_weight = sigmoid(bsum)

    def row_target(q, step):
        pp = floor_div(q, erow)
        rem = q - pp * erow
        zz = floor_div(rem, cap)
        return jnp.where(zz < zs_n, zz * step + pp * cap + (rem - zz * cap), -1e6)

    def permutation(rows, slots, step, shift):
        q = lax.broadcasted_iota(jnp.int32, (rows, slots), 0).astype(f32)
        t = lax.broadcasted_iota(jnp.int32, (rows, slots), 1).astype(f32)
        return jnp.where(row_target(q, step) + shift == t, 1.0, 0.0).astype(bf16)

    for cc in range(parts):
        perms[cc] = permutation(erow, slots, arow, 1.0 * cc * cap)
    wsend[...] = pack(last, wide_source, wide_lanes)
    wrecv[z] = wsend[z]

    def unpermutation(rows, slots, step, shift):
        q = lax.broadcasted_iota(jnp.int32, (slots, rows), 1).astype(f32)
        t = lax.broadcasted_iota(jnp.int32, (slots, rows), 0).astype(f32)
        return jnp.where(row_target(q, step) + shift == t, 1.0, 0.0).astype(bf16)

    east, west = at(z, y, c, xpeer(1)), at(z, y, c, xpeer(xs_n - 1))
    partner = at(z, y, 1 - c, x)
    mate = at(z, y + 1 - 2 * h, c, x)
    started, bz, bx, backs_z, returned = [], [], [], [], []
    pending = {}

    def begin(copy):
        copy.start()
        started.append(copy)
        return copy

    def tok_part(k, xx):
        return tok.at[k, c, :, pl.ds(pl.multiple_of(xx * dx, dx), dx)]

    def hid_part(k, xx):
        return hid.at[k, :, :, pl.ds(pl.multiple_of(xx * fx, fx), fx)]

    def spread(part, sems, rsems, k):
        for way, dev in ((0, east), (1, west)):
            begin(remote(part(k, x), part(k, x), sems.at[0], rsems.at[way, k], dev))

    def arrive(part, rsems, sems, way, k):
        ref = part(k, x)
        remote(ref, ref, sems.at[0], rsems.at[way, k], east).wait_recv()

    def relay(part, sems, rsems, k):
        way = lax.rem(k, 2)
        arrive(part, rsems, sems, way, k)
        ref = part(k, xpeer(xs_n - 1 - 2 * way))
        dev = at(z, y, c, xpeer(1 + 2 * way))
        begin(remote(ref, ref, sems.at[0], rsems.at[2, k], dev))

    def settle(part, sems, rsems, k):
        arrive(part, rsems, sems, 1 - k % 2, k)
        arrive(part, rsems, sems, 2, k)

    def y_wait(k):
        ref = tok.at[k, c, :, own_cols]
        remote(ref, ref, yd_s.at[0], yd_r.at[k], mate).wait_recv()

    def both(i):
        return (2 * i, 2 * i + 1)

    def step_d(i):
        with jax.named_scope(f"z_wait{i}"):
            if near:
                zd_all(i).wait_recv()
        rows = zrecv[i].reshape(slots, lanes)
        for cc in range(parts):
            moved = jnp.dot(perms[cc], rows, preferred_element_type=f32)
            ysend[i, :, cc * lanes : (cc + 1) * lanes] = moved.astype(bf16)
        pt = lax.rem(pair + pairs + offset[i] * (1 - 2 * h), pairs)
        near_chip = lax.rem(h + hops[i], 2)
        k = 2 * i + near_chip
        for n, hh in enumerate((near_chip, 1 - near_chip)):
            if hops[i] > 1 and n == 1:
                break
            dst = tok.at[k, c, :, own_cols]
            dev = at(z, 2 * pt + hh, c, x)
            begin(remote(ysend.at[i], dst, yd_s.at[0], yd_r.at[k], dev))
        if i + 2 <= last:
            z_send(i + 2)

    def to_partner(k, ref):
        begin(remote(ref, ref, tc_s.at[0], tc_r.at[k], partner))

    def step_o(part):
        mine = 2 * last + h
        if part == 1:
            with jax.named_scope("z_wait_wide"):
                if near:
                    zd_all(last).wait_recv()
            rows = wrecv[...].reshape(slots, wide_lanes)
            for cc in range(parts):
                moved = jnp.dot(perms[cc], rows, preferred_element_type=f32)
                cols = slice(cc * wide_lanes, (cc + 1) * wide_lanes)
                tok[mine, c, :, cols] = moved.astype(bf16)
            ref = tok.at[mine, c]
            begin(remote(ref, ref, yd_s.at[0], yd_r.at[mine], mate))
            to_partner(mine, ref)
            return
        ref = tok.at[2 * last + 1 - h, c]
        with jax.named_scope("wide_mate"):
            remote(ref, ref, yd_s.at[0], yd_r.at[2 * last + 1 - h], mate).wait_recv()
        to_partner(2 * last + 1 - h, ref)

    def by_all():
        ref = bw.at[:, 0, pl.ds(0, zs_n - 1), 0]
        return remote(ref, ref, by_s.at[0], by_r.at[0], partner)

    def bz_all():
        ref = bw.at[:, :, pl.ds(0, ys_n - 1), 0]
        return remote(ref, ref, bz_s.at[0], bz_r.at[0], partner)

    def bx_all():
        ref = bgot.at[pl.ds(0, xs_n - 1)]
        return remote(ref, ref, bx_s.at[0], bx_r.at[0], partner)

    def branch_planes():
        if near:
            by_all().wait_recv()
        for r in range(1, ys_n):
            part = bw.at[:, :, y, c]
            copy = remote(part, part, bz_s.at[0], bz_r.at[0], at(z, ypeer(r), c, x))
            copy.start()
            bz.append(copy)

    def step_n(i):
        mine = 2 * i + h
        with jax.named_scope(f"n_wait{i}"):
            y_wait(mine)
        if hops[i] > 1:
            ref = tok.at[mine, c, :, own_cols]
            begin(remote(ref, ref, yd_s.at[0], yd_r.at[mine], mate))
        spread(tok_part, tx_s, tx_r, mine)
        to_partner(mine, tok_part(mine, x))

    def step_m(i):
        with jax.named_scope(f"m_wait{i}"):
            y_wait(2 * i + 1 - h)
        k = 2 * i + 1 - h
        spread(tok_part, tx_s, tx_r, k)
        to_partner(k, tok_part(k, x))

    def step_b(i):
        for n, k in enumerate((2 * i + h, 2 * i + 1 - h)):
            with jax.named_scope(f"b_relay{i}_{n}"):
                relay(tok_part, tx_s, tx_r, k)
            to_partner(k, tok_part(k, xpeer(xs_n - 1 - 2 * lax.rem(k, 2))))

    def step_c(i):
        for k in both(i):
            way = k % 2
            with jax.named_scope(f"c_settle{k}"):
                arrive(tok_part, tx_r, tx_s, 1 - way, k)
            to_partner(k, tok_part(k, xpeer(1 + 2 * way)))
        for k in both(i):
            with jax.named_scope(f"c_last{k}"):
                arrive(tok_part, tx_r, tx_s, 2, k)
            to_partner(k, tok_part(k, xpeer(2)))

    def step_e(i):
        with jax.named_scope(f"e_wait{i}"):
            for k in both(i):
                ref = tok.at[k, 1 - c]
                remote(ref, ref, tc_s.at[0], tc_r.at[k], partner).wait_recv()
            while len(weights) > 1:
                weights.pop(0).wait()
        with jax.named_scope(f"e_dot{i}"):
            rows = tok[2 * i : 2 * i + 2].reshape(2 * CORES * erow, width)
            pre = jnp.dot(rows, w_gu[...], preferred_element_type=f32)
            gate, up = pre[:, :fx], pre[:, fx:]
            hidden = (gate / (1.0 + jnp.exp(-gate)) * up).astype(bf16)
            cols = pl.ds(pl.multiple_of(x * fx, fx), fx)
            hid[2 * i : 2 * i + 2, :, :, cols] = hidden.reshape(2, CORES, erow, fx)
        for k in both(i):
            spread(hid_part, hx_s, hx_r, k)

    def step_f(i):
        for k in both(i):
            with jax.named_scope(f"f_relay{k}"):
                relay(hid_part, hx_s, hx_r, k)

    def step_g(i):
        for k in both(i):
            with jax.named_scope(f"g_settle{k}"):
                settle(hid_part, hx_s, hx_r, k)
        while weights:
            weights.pop(0).wait()
        with jax.named_scope(f"g_dot{i}"):
            rows = hid[2 * i : 2 * i + 2].reshape(2 * CORES * erow, hid.shape[3])
            part = jnp.dot(rows, w_dn[...], preferred_element_type=f32)
            part = part.reshape(2, CORES, erow, dx)
            acc[i] = part
            psend[2 * i : 2 * i + 2] = part.astype(bf16)
        two = pl.ds(2 * i, 2)
        pending["g", i] = begin(
            remote(psend.at[two, 1 - c], precv.at[two], pc_s.at[0], pc_r.at[i], partner)
        )

    def step_i(i):
        with jax.named_scope(f"i_wait{i}"):
            pending["g", i].wait_recv()
        total = acc[i, :, c] + precv[2 * i : 2 * i + 2].astype(f32)
        fsend[2 * i : 2 * i + 2] = total.astype(bf16)
        if i == last:
            yback[i, h] = fsend[2 * i + h]
            src = fsend.at[2 * i + 1 - h]
            begin(remote(src, yback.at[i, h], fy_s.at[0], fy_r.at[i, h], mate))
            return
        if i == far:
            half[...] = total
            copy = remote(fsend.at[2 * i + 1 - h], qrecv, qy_s.at[0], qy_r.at[0], mate)
            pending["i", i] = begin(copy)
            return
        for side in (0, 1):
            way = hops[i] + 1 if side else ys_n - hops[i]
            back = at(z, lax.rem(2 * pair + way, ys_n), c, x)
            k = 2 * i + side
            begin(remote(fsend.at[k], yback.at[i, h], fy_s.at[0], fy_r.at[i, h], back))

    def step_j(i):
        with jax.named_scope(f"j_wait{i}"):
            pending["i", i].wait_recv()
        fsend[2 * i + h] = (half[h] + qrecv[...].astype(f32)).astype(bf16)
        back = at(z, lax.rem(y + ys_n + hops[i] * (2 * h - 1), ys_n), c, x)
        k = 2 * i + h
        begin(remote(fsend.at[k], yback.at[i, 0], fy_s.at[0], fy_r.at[i, 0], back))

    def back_wait(i, hh):
        ref = yback.at[i, hh]
        remote(ref, ref, fy_s.at[0], fy_r.at[i, hh], mate).wait_recv()

    def zb_all(n):
        base = sum(g_rows[:n])
        ref = zgot.at[pl.ds(0, zs_n - 1), pl.ds(base, g_rows[n])]
        return remote(ref, ref, zb_s.at[n], zb_r.at[n], partner)

    def z_return(n):
        group, step = groups[n], g_rows[n]
        many = len(group) * erow
        perms = [
            unpermutation(many, zs_n * step, step, 1.0 * cc * len(group) * cap)
            for cc in range(parts)
        ]
        with jax.named_scope(f"back_wait{n}"):
            for i in group:
                if i == last:
                    back_wait(i, 1 - h)
                elif i == far:
                    back_wait(i, 0)
                else:
                    back_wait(i, 0)
                    back_wait(i, 1)
        moved = 0.0
        for hh in (0,) if group == [far] else (0, 1):
            rows = yback[group[0] : group[-1] + 1, hh].reshape(many, dx)
            for cc, perm in enumerate(perms):
                piece = rows[:, cc * lanes : (cc + 1) * lanes]
                moved = moved + jnp.dot(perm, piece, preferred_element_type=f32)
        base = sum(g_rows[:n])
        zback[:, base : base + step] = moved.astype(bf16).reshape(zs_n, step, lanes)
        rows = pl.ds(base, step)
        kept = []
        for r in near:
            zt = zpeer(r)
            copy = remote(
                zback.at[zt, rows], zgot.at[z, rows], zb_s.at[n], zb_r.at[n], at(zt, y, c, x)
            )
            copy.start()
            kept.append(copy)
        zgot[z, base : base + step] = zback[z, base : base + step]
        backs_z.extend(kept)
        returned.append((n, kept))

    def branch_core():
        with jax.named_scope("bz_wait"):
            bz_all().wait_recv()
        begin(remote(bw.at[:, :, :, c], bw.at[:, :, :, c], bc_s.at[0], bc_r.at[0], partner))

    def branch_dense():
        ref = bw.at[:, :, :, 1 - c]
        remote(ref, ref, bc_s.at[0], bc_r.at[0], partner).wait_recv()
        whole_in = bw[0].reshape(width, bw.shape[5])
        pre = jnp.dot(normed[...], whole_in, preferred_element_type=f32)
        hb = (pre / (1.0 + jnp.exp(-pre))).astype(bf16)
        for xx in range(xs_n):
            zpart = zs_n // xs_n if zs_n >= xs_n else 0
            if zpart:
                wo = bw[1, xx * zpart : (xx + 1) * zpart].reshape(dx, bw.shape[5])
            else:
                wo = bw[1].reshape(width, bw.shape[5])[xx * dx : (xx + 1) * dx]
            term = lax.dot_general(hb, wo, (((1,), (1,)), ((), ())), preferred_element_type=f32)
            bterm[xx] = term.astype(bf16)

    def branch_send():
        for r in range(1, xs_n):
            xt = xpeer(r)
            copy = remote(bterm.at[xt], bgot.at[r], bx_s.at[0], bx_r.at[0], at(z, y, c, xt))
            copy.start()
            bx.append(copy)

    order = ("d0", "d1", "n0", "m0", "d2", "n1", "b0", "m1", "n2", "c0", "b1", "o1", "m2", "planes", "e0", "b2", "c1", "e1", "c2", "e2", "f1", "f0", "o2", "e3", "f2", "g1", "i1", "g2", "g0", "core", "i2", "i0", "f3", "dense", "j2", "g3", "i3", "z0", "send", "z2", "z1")
    steps = dict(b=step_b, c=step_c, d=step_d, e=step_e, f=step_f, g=step_g, i=step_i, j=step_j)
    steps.update(m=step_m, n=step_n, o=step_o, z=z_return)
    others = dict(planes=branch_planes, core=branch_core, dense=branch_dense, send=branch_send)
    for item in order:
        if item in others:
            others[item]()
        else:
            steps[item[0]](int(item[1]))

    diff = scores_t[0:1, :] - scores_t[1:2, :]
    mixes = []
    for d in (diff, -diff):
        row = jnp.broadcast_to(sigmoid(d), sq)
        mixes.append(jnp.sum(jnp.where(sq_a == sq_b, row, 0.0), axis=1, keepdims=True))

    def column(row):
        wide_row = jnp.broadcast_to(row, sq)
        return jnp.sum(jnp.where(sq_a == sq_b, wide_row, 0.0), axis=1, keepdims=True)

    spots = [column(come[r]) for r in (0, 1)]

    def picks(n):
        shape = (rows_tok, zs_n * g_rows[n])
        t = lax.broadcasted_iota(jnp.int32, shape, 1).astype(f32) + 1.0 * g_low[n]
        size = len(groups[n]) * cap
        return [
            [jnp.where(t == spots[r] + 1.0 * cc * size, 1.0, 0.0).astype(bf16) for cc in range(parts)]
            for r in (0, 1)
        ]

    def combine(n, taken):
        base = sum(g_rows[:n])
        rows = zgot[:, base : base + g_rows[n]].reshape(zs_n * g_rows[n], lanes)
        terms = []
        for cc in range(parts):
            one = jnp.dot(taken[0][cc], rows, preferred_element_type=f32)
            two = jnp.dot(taken[1][cc], rows, preferred_element_type=f32)
            terms.append(mixes[0] * one + mixes[1] * two)
        return jnp.concatenate(terms, axis=1)

    with jax.named_scope("bx_wait"):
        bx_all().wait_recv()
    share = bterm[x].astype(f32)
    for r in range(1, xs_n):
        share = share + bgot[r].astype(f32)
    share = share * branch_weight
    for n, _ in returned:
        taken = picks(n)
        with jax.named_scope(f"kept{n}"):
            if near:
                zb_all(n).wait_recv()
        share = share + combine(n, taken)
    out[...] = share.astype(out.dtype)

    with jax.named_scope("send_wait"):
        if near:
            for i in range(1, pairs):
                zd_all(i).wait_send()
            for n in range(len(groups)):
                zb_all(n).wait_send()
            by_all().wait_send()
        bz_all().wait_send()
        bx_all().wait_send()
        narrow = 2 * last
        for ref, sem in (
            (tok.at[pl.ds(0, last), :, :, pl.ds(0, 3 * dx)], tx_s),
            (hid.at[:, :, :, pl.ds(0, 3 * fx)], hx_s),
            (tok.at[:, 0], tc_s),
            (tok.at[pl.ds(0, last + 2), :, :, pl.ds(0, dx)], yd_s),
            (fsend.at[pl.ds(0, narrow)], fy_s),
            (psend.at[:, 0], pc_s),
            (qrecv, qy_s),
            (bw.at[:, :, :, 0], bc_s),
        ):
            remote(ref, ref, sem.at[0], qy_r.at[0], partner).wait_send()


def on_device(
    cores_z,
    cores_y,
    tokens,
    norm_gain,
    routes,
    route_scores,
    expert_gate,
    expert_up,
    expert_down,
    branch_in,
    branch_out,
    branch_gate,
):
    zs_n, ys_n = cores_z, cores_y
    xs_n = lax.axis_size("tp")
    rows_tok, width = tokens.shape
    experts = zs_n * ys_n // 2
    cap = 5 * rows_tok * routes.shape[1] // (4 * experts)
    pairs = ys_n // 2
    dx = width // xs_n
    fx = expert_gate.shape[2]
    fg = expert_down.shape[1]
    arow = round_up(dx // 128 * cap, 16)
    erow = round_up(zs_n * cap, 16)
    back_rows = sum(round_up(dx // 128 * len(g) * cap, 16) for g in return_groups(pairs))
    bpart = branch_in.shape
    bf16, f32 = jnp.bfloat16, jnp.float32
    vm = lambda shape, dtype=bf16: pltpu.VMEM(shape, dtype)
    sem = lambda *shape: pltpu.SemaphoreType.DMA(shape)
    scratch = [
        vm((rows_tok, width)),
        vm((1, width), f32),
        vm((2, rows_tok), jnp.int32),
        vm((2, rows_tok), f32),
        vm((1, width), f32),
        vm(bpart),
        vm(bpart),
        vm((rows_tok, width)),
        vm((pairs - 1, zs_n, arow, 128)),
        vm((pairs - 1, zs_n, arow, 128)),
        vm((zs_n, arow, width // (dx // 128))),
        vm((zs_n, arow, width // (dx // 128))),
        vm((pairs - 1, erow, dx)),
        vm((ys_n, CORES, erow, width)),
        vm((width, 2 * fx)),
        vm((fg, dx)),
        vm((ys_n, CORES, erow, fg)),
        vm((pairs, 2, CORES, erow, dx), f32),
        vm((ys_n, CORES, erow, dx)),
        vm((ys_n, erow, dx)),
        vm((dx // 128, erow, zs_n * arow)),
        vm((2, erow, dx), f32),
        vm((erow, dx)),
        vm((ys_n, erow, dx)),
        vm((pairs, 2, erow, dx)),
        vm((zs_n, back_rows, 128)),
        vm((zs_n, back_rows, 128)),
        vm((2, zs_n, ys_n, CORES, *bpart)),
        vm((xs_n, rows_tok, dx)),
        vm((xs_n, rows_tok, dx)),
        sem(10),
        sem(pairs),
        sem(pairs),
        sem(1),
        sem(ys_n),
        sem(1),
        sem(3, ys_n),
        sem(1),
        sem(ys_n),
        sem(1),
        sem(3, ys_n),
        sem(1),
        sem(pairs),
        sem(1),
        sem(1),
        sem(1),
        sem(pairs, 2),
        sem(pairs),
        sem(pairs),
        sem(1),
        sem(1),
        sem(1),
        sem(1),
        sem(1),
        sem(1),
        sem(1),
        sem(1),
    ]
    in_vmem = pl.BlockSpec(memory_space=pltpu.VMEM)
    in_hbm = pl.BlockSpec(memory_space=pl.ANY)
    return pl.pallas_call(
        functools.partial(layer_kernel, zs_n, ys_n, xs_n, cap),
        out_shape=jax.ShapeDtypeStruct((rows_tok, dx), bf16),
        in_specs=[in_hbm] * 10,
        out_specs=in_vmem,
        scratch_shapes=scratch,
        compiler_params=pltpu.CompilerParams(
            collective_id=0, has_side_effects=True, vmem_limit_bytes=60 * 1024 * 1024
        ),
        name="routed_layer",
    )(
        tokens,
        norm_gain.reshape(1, -1),
        routes.T,
        route_scores.T,
        branch_gate.reshape(1, -1),
        branch_in,
        branch_out.T,
        expert_gate,
        expert_up,
        expert_down,
    )


def solution(mesh, z_y=None):
    ep = mesh.shape["ep"]
    zs_n, ys_n = z_y or (8, ep // (8 * CORES))
    in_specs = (
        P("ep", None),
        P(),
        P("ep", None),
        P("ep", None),
        P("ep", None, "tp"),
        P("ep", None, "tp"),
        P("ep", None, "tp"),
        P("ep", "tp"),
        P("tp", "ep"),
        P(),
    )
    return jax.shard_map(
        functools.partial(on_device, zs_n, ys_n),
        mesh=mesh,
        in_specs=in_specs,
        out_specs=P("ep", "tp"),
        check_vma=False,
    )
```

```python
import functools

import jax
import jax.numpy as jnp
from jax import lax
from jax.experimental import pallas as pl
from jax.experimental.pallas import tpu as pltpu
from jax.sharding import PartitionSpec as P

NORM_EPSILON = 1e-06
GROUP = 4
CORES = 2
MESH_ID = pl.DeviceIdType.MESH


def round_up(n, m):
    return (n + m - 1) // m * m


def sigmoid(v):
    return 1.0 / (1.0 + jnp.exp(-v))


def floor_div(v, n):
    return jnp.floor((v + 0.5) * (1.0 / n))


def return_groups(pairs):
    return [[0, 1], [2], [3]] if pairs == 4 else [[i] for i in range(pairs)]


def layer_kernel(
    zs_n,
    ys_n,
    xs_n,
    cap,
    tokens_h,
    gain_h,
    routes_h,
    scores_h,
    bgate_h,
    b_in_h,
    b_out_h,
    w_gate,
    w_up,
    w_down,
    out,
    tokens,
    gain,
    routes_t,
    scores_t,
    bgate,
    b_in,
    b_out,
    normed,
    zsend,
    zrecv,
    wsend,
    wrecv,
    ysend,
    tok,
    w_gu,
    w_dn,
    hid,
    acc,
    psend,
    precv,
    perms,
    half,
    qrecv,
    fsend,
    yback,
    zback,
    zgot,
    bw,
    bterm,
    bgot,
    local_sem,
    zd_s,
    zd_r,
    yd_s,
    yd_r,
    tx_s,
    tx_r,
    tc_s,
    tc_r,
    hx_s,
    hx_r,
    pc_s,
    pc_r,
    qy_s,
    qy_r,
    fy_s,
    fy_r,
    zb_s,
    zb_r,
    by_s,
    by_r,
    bz_s,
    bz_r,
    bc_s,
    bc_r,
    bx_s,
    bx_r,
):
    f32, bf16 = jnp.float32, jnp.bfloat16
    ep = lax.axis_index("ep")
    x = lax.axis_index("tp")
    c = lax.rem(ep, CORES)
    y = lax.rem(ep // CORES, ys_n)
    z = ep // (CORES * ys_n)
    pairs = ys_n // 2
    pair = y // 2
    h = lax.rem(y, 2)
    hops = list(range(1, pairs)) + [0]
    last = pairs - 1
    offset = [last] + list(range(1, last)) + [0]
    rows_tok, width = tokens.shape
    dx = width // xs_n
    fx = w_gate.shape[2]
    groups = return_groups(pairs)
    lanes = 128
    parts = dx // lanes
    g_rows = [round_up(parts * len(g) * cap, 16) for g in groups]
    g_low = [zs_n * sum(g_rows[:n]) for n in range(len(groups))]
    experts = zs_n * pairs
    arow = zsend.shape[2]
    slots = zs_n * arow
    erow = ysend.shape[1]
    far = hops.index(last)

    def at(z_, y_, c_, x_):
        return ((z_ * ys_n + y_) * CORES + c_, x_)

    def zpeer(r):
        return lax.rem(z + r, zs_n)

    def ypeer(r):
        return lax.rem(y + r, ys_n)

    def xpeer(r):
        return lax.rem(x + r, xs_n)

    def remote(src, dst, s, r, dev):
        return pltpu.make_async_remote_copy(
            src_ref=src, dst_ref=dst, send_sem=s, recv_sem=r, device_id=dev, device_id_type=MESH_ID
        )

    barrier = pltpu.get_barrier_semaphore()
    peers = [at(zpeer(r), y, c, x) for r in range(1, zs_n)]
    peers += [at(z, ypeer(r), c, x) for r in range(1, ys_n)]
    peers += [at(z, y, c, xpeer(r)) for r in range(1, xs_n)]
    peers += [at(z, y, 1 - c, x)]
    for dev in peers:
        pl.semaphore_signal(barrier, inc=1, device_id=dev, device_id_type=MESH_ID)

    pairs_in = (
        (tokens_h, tokens),
        (routes_h, routes_t),
        (gain_h, gain),
        (b_in_h, b_in),
        (b_out_h, b_out),
        (bgate_h, bgate),
        (scores_h, scores_t),
    )
    fetched = [
        pltpu.make_async_copy(src, dst, local_sem.at[3 + n])
        for n, (src, dst) in enumerate(pairs_in)
    ]
    for copy in fetched:
        copy.start()
    weights = [
        pltpu.make_async_copy(w_gate.at[0], w_gu.at[:, pl.ds(0, fx)], local_sem.at[0]),
        pltpu.make_async_copy(w_up.at[0], w_gu.at[:, pl.ds(fx, fx)], local_sem.at[1]),
        pltpu.make_async_copy(w_down.at[0], w_dn, local_sem.at[2]),
    ]
    for copy in weights:
        copy.start()

    for copy in fetched:
        copy.wait()
    tf = tokens[...].astype(f32)
    scaled = lax.rsqrt(jnp.sum(tf * tf, axis=-1, keepdims=True) * (1.0 / width) + NORM_EPSILON)
    nf = (tf * scaled * gain[...]).astype(bf16)
    normed[...] = nf

    ids = lax.broadcasted_iota(jnp.int32, (experts, rows_tok), 0)
    sq = (rows_tok, rows_tok)
    sq_a = lax.broadcasted_iota(jnp.int32, sq, 0)
    sq_b = lax.broadcasted_iota(jnp.int32, sq, 1)
    chosen = [jnp.where(ids == routes_t[r : r + 1, :], 1.0, 0.0) for r in (0, 1)]
    earlier = jnp.where(sq_a < sq_b, 1.0, 0.0).astype(bf16)
    ranks = jnp.dot((chosen[0] + chosen[1]).astype(bf16), earlier, preferred_element_type=f32)
    go, come = [], []
    for r in (0, 1):
        rank = jnp.sum(chosen[r] * ranks, axis=0, keepdims=True)
        e = routes_t[r : r + 1, :].astype(f32)
        zz = floor_div(e, pairs)
        v = (e - zz * pairs - pair.astype(f32)) * (1 - 2 * h).astype(f32) + pairs
        rel = jnp.where(v >= pairs, v - pairs, v)
        rel = jnp.where(rel < 0.5, 1.0 * last, jnp.where(rel > last - 0.5, 0.0, rel))
        go.append(rank + rel * slots + zz * arow)
        place = 0.0
        for group, n_rows, low in zip(groups, g_rows, g_low):
            spot = low + zz * n_rows + (rel - group[0]) * cap
            place = spot if group[0] == 0 else jnp.where(rel > group[0] - 0.5, spot, place)
        come.append(rank + place)
    own_cols = pl.ds(pl.multiple_of(x * dx, dx), dx)
    wide_lanes = width // parts

    def pack(i, source, n_lanes):
        srow = lax.broadcasted_iota(jnp.int32, (slots, rows_tok), 0).astype(f32) + 1.0 * i * slots
        total = 0.0
        for cc in range(parts):
            here = srow - 1.0 * cc * cap
            pick = jnp.where((here == go[0]) | (here == go[1]), 1.0, 0.0).astype(bf16)
            total = total + jnp.dot(pick, source(cc), preferred_element_type=f32)
        return total.astype(bf16).reshape(zs_n, arow, n_lanes)

    def narrow_source(cc):
        start = pl.multiple_of(x * dx + cc * lanes, lanes)
        return normed[:, pl.ds(start, lanes)]

    def wide_source(cc):
        return normed[:, cc * wide_lanes : (cc + 1) * wide_lanes]

    zsend[0] = pack(0, narrow_source, lanes)

    pl.semaphore_wait(barrier, len(peers))

    zd, by = {}, []
    near = sorted(range(1, zs_n), key=lambda r: min(r, zs_n - r))

    def z_send(i):
        src, dst = (wsend, wrecv) if i == last else (zsend.at[i], zrecv.at[i])
        zd[i] = []
        for r in near:
            zt = zpeer(r)
            copy = remote(src.at[zt], dst.at[z], zd_s.at[i], zd_r.at[i], at(zt, y, c, x))
            copy.start()
            zd[i].append(copy)

    def zd_all(i):
        ref = wrecv if i == last else zrecv.at[i]
        ref = ref.at[pl.ds(0, zs_n - 1)]
        return remote(ref, ref, zd_s.at[i], zd_r.at[i], at(z, y, 1 - c, x))

    z_send(0)
    for i in range(1, last):
        zsend[i] = pack(i, narrow_source, lanes)
    for i in range(last):
        zrecv[i, z] = zsend[i, z]
    if near:
        zd_all(0).wait_send()
    z_send(1)
    for r in near:
        for w, part in enumerate((b_in, b_out)):
            copy = remote(
                part, bw.at[w, z, y, c], by_s.at[0], by_r.at[0], at(zpeer(r), y, c, x)
            )
            copy.start()
            by.append(copy)
    bw[0, z, y, c] = b_in[...]
    bw[1, z, y, c] = b_out[...]

    bsum = jnp.sum(normed[...].astype(f32) * bgate[...], axis=-1, keepdims=True)
    branch_weight = sigmoid(bsum)

    def row_target(q, step):
        pp = floor_div(q, erow)
        rem = q - pp * erow
        zz = floor_div(rem, cap)
        return jnp.where(zz < zs_n, zz * step + pp * cap + (rem - zz * cap), -1e6)

    def permutation(rows, slots, step, shift):
        q = lax.broadcasted_iota(jnp.int32, (rows, slots), 0).astype(f32)
        t = lax.broadcasted_iota(jnp.int32, (rows, slots), 1).astype(f32)
        return jnp.where(row_target(q, step) + shift == t, 1.0, 0.0).astype(bf16)

    for cc in range(parts):
        perms[cc] = permutation(erow, slots, arow, 1.0 * cc * cap)
    wsend[...] = pack(last, wide_source, wide_lanes)
    wrecv[z] = wsend[z]

    def unpermutation(rows, slots, step, shift):
        q = lax.broadcasted_iota(jnp.int32, (slots, rows), 1).astype(f32)
        t = lax.broadcasted_iota(jnp.int32, (slots, rows), 0).astype(f32)
        return jnp.where(row_target(q, step) + shift == t, 1.0, 0.0).astype(bf16)

    east, west = at(z, y, c, xpeer(1)), at(z, y, c, xpeer(xs_n - 1))
    partner = at(z, y, 1 - c, x)
    mate = at(z, y + 1 - 2 * h, c, x)
    started, bz, bx, backs_z, returned = [], [], [], [], []
    pending = {}

    def begin(copy):
        copy.start()
        started.append(copy)
        return copy

    def tok_part(k, xx):
        return tok.at[k, c, :, pl.ds(pl.multiple_of(xx * dx, dx), dx)]

    def hid_part(k, xx):
        return hid.at[k, :, :, pl.ds(pl.multiple_of(xx * fx, fx), fx)]

    def spread(part, sems, rsems, k):
        for way, dev in ((0, east), (1, west)):
            begin(remote(part(k, x), part(k, x), sems.at[0], rsems.at[way, k], dev))

    def arrive(part, rsems, sems, way, k):
        ref = part(k, x)
        remote(ref, ref, sems.at[0], rsems.at[way, k], east).wait_recv()

    def relay(part, sems, rsems, k):
        way = lax.rem(k, 2)
        arrive(part, rsems, sems, way, k)
        ref = part(k, xpeer(xs_n - 1 - 2 * way))
        dev = at(z, y, c, xpeer(1 + 2 * way))
        begin(remote(ref, ref, sems.at[0], rsems.at[2, k], dev))

    def settle(part, sems, rsems, k):
        arrive(part, rsems, sems, 1 - k % 2, k)
        arrive(part, rsems, sems, 2, k)

    def y_wait(k):
        ref = tok.at[k, c, :, own_cols]
        remote(ref, ref, yd_s.at[0], yd_r.at[k], mate).wait_recv()

    def both(i):
        return (2 * i, 2 * i + 1)

    def step_d(i):
        with jax.named_scope(f"z_wait{i}"):
            if near:
                zd_all(i).wait_recv()
        rows = zrecv[i].reshape(slots, lanes)
        for cc in range(parts):
            moved = jnp.dot(perms[cc], rows, preferred_element_type=f32)
            ysend[i, :, cc * lanes : (cc + 1) * lanes] = moved.astype(bf16)
        pt = lax.rem(pair + pairs + offset[i] * (1 - 2 * h), pairs)
        near_chip = lax.rem(h + hops[i], 2)
        k = 2 * i + near_chip
        for n, hh in enumerate((near_chip, 1 - near_chip)):
            if hops[i] > 1 and n == 1:
                break
            dst = tok.at[k, c, :, own_cols]
            dev = at(z, 2 * pt + hh, c, x)
            begin(remote(ysend.at[i], dst, yd_s.at[0], yd_r.at[k], dev))
        if i + 2 <= last:
            z_send(i + 2)

    def to_partner(k, ref):
        begin(remote(ref, ref, tc_s.at[0], tc_r.at[k], partner))

    def step_o(part):
        mine = 2 * last + h
        if part == 1:
            with jax.named_scope("z_wait_wide"):
                if near:
                    zd_all(last).wait_recv()
            rows = wrecv[...].reshape(slots, wide_lanes)
            for cc in range(parts):
                moved = jnp.dot(perms[cc], rows, preferred_element_type=f32)
                cols = slice(cc * wide_lanes, (cc + 1) * wide_lanes)
                tok[mine, c, :, cols] = moved.astype(bf16)
            ref = tok.at[mine, c]
            begin(remote(ref, ref, yd_s.at[0], yd_r.at[mine], mate))
            to_partner(mine, ref)
            return
        ref = tok.at[2 * last + 1 - h, c]
        with jax.named_scope("wide_mate"):
            remote(ref, ref, yd_s.at[0], yd_r.at[2 * last + 1 - h], mate).wait_recv()
        to_partner(2 * last + 1 - h, ref)

    def by_all():
        ref = bw.at[:, 0, pl.ds(0, zs_n - 1), 0]
        return remote(ref, ref, by_s.at[0], by_r.at[0], partner)

    def bz_all():
        ref = bw.at[:, :, pl.ds(0, ys_n - 1), 0]
        return remote(ref, ref, bz_s.at[0], bz_r.at[0], partner)

    def bx_all():
        ref = bgot.at[pl.ds(0, xs_n - 1)]
        return remote(ref, ref, bx_s.at[0], bx_r.at[0], partner)

    def branch_planes():
        if near:
            by_all().wait_recv()
        for r in range(1, ys_n):
            part = bw.at[:, :, y, c]
            copy = remote(part, part, bz_s.at[0], bz_r.at[0], at(z, ypeer(r), c, x))
            copy.start()
            bz.append(copy)

    def step_n(i):
        mine = 2 * i + h
        with jax.named_scope(f"n_wait{i}"):
            y_wait(mine)
        if hops[i] > 1:
            ref = tok.at[mine, c, :, own_cols]
            begin(remote(ref, ref, yd_s.at[0], yd_r.at[mine], mate))
        spread(tok_part, tx_s, tx_r, mine)
        to_partner(mine, tok_part(mine, x))

    def step_m(i):
        with jax.named_scope(f"m_wait{i}"):
            y_wait(2 * i + 1 - h)
        k = 2 * i + 1 - h
        spread(tok_part, tx_s, tx_r, k)
        to_partner(k, tok_part(k, x))

    def step_b(i):
        for n, k in enumerate((2 * i + h, 2 * i + 1 - h)):
            with jax.named_scope(f"b_relay{i}_{n}"):
                relay(tok_part, tx_s, tx_r, k)
            to_partner(k, tok_part(k, xpeer(xs_n - 1 - 2 * lax.rem(k, 2))))

    def step_c(i):
        for k in both(i):
            way = k % 2
            with jax.named_scope(f"c_settle{k}"):
                arrive(tok_part, tx_r, tx_s, 1 - way, k)
            to_partner(k, tok_part(k, xpeer(1 + 2 * way)))
        for k in both(i):
            with jax.named_scope(f"c_last{k}"):
                arrive(tok_part, tx_r, tx_s, 2, k)
            to_partner(k, tok_part(k, xpeer(2)))

    def step_e(i):
        with jax.named_scope(f"e_wait{i}"):
            for k in both(i):
                ref = tok.at[k, 1 - c]
                remote(ref, ref, tc_s.at[0], tc_r.at[k], partner).wait_recv()
            while len(weights) > 1:
                weights.pop(0).wait()
        with jax.named_scope(f"e_dot{i}"):
            rows = tok[2 * i : 2 * i + 2].reshape(2 * CORES * erow, width)
            pre = jnp.dot(rows, w_gu[...], preferred_element_type=f32)
            gate, up = pre[:, :fx], pre[:, fx:]
            hidden = (gate / (1.0 + jnp.exp(-gate)) * up).astype(bf16)
            cols = pl.ds(pl.multiple_of(x * fx, fx), fx)
            hid[2 * i : 2 * i + 2, :, :, cols] = hidden.reshape(2, CORES, erow, fx)
        for k in both(i):
            spread(hid_part, hx_s, hx_r, k)

    def step_f(i):
        for k in both(i):
            with jax.named_scope(f"f_relay{k}"):
                relay(hid_part, hx_s, hx_r, k)

    def step_g(i):
        for k in both(i):
            with jax.named_scope(f"g_settle{k}"):
                settle(hid_part, hx_s, hx_r, k)
        while weights:
            weights.pop(0).wait()
        with jax.named_scope(f"g_dot{i}"):
            rows = hid[2 * i : 2 * i + 2].reshape(2 * CORES * erow, hid.shape[3])
            part = jnp.dot(rows, w_dn[...], preferred_element_type=f32)
            part = part.reshape(2, CORES, erow, dx)
            acc[i] = part
            psend[2 * i : 2 * i + 2] = part.astype(bf16)
        two = pl.ds(2 * i, 2)
        pending["g", i] = begin(
            remote(psend.at[two, 1 - c], precv.at[two], pc_s.at[0], pc_r.at[i], partner)
        )

    def step_i(i):
        with jax.named_scope(f"i_wait{i}"):
            pending["g", i].wait_recv()
        total = acc[i, :, c] + precv[2 * i : 2 * i + 2].astype(f32)
        fsend[2 * i : 2 * i + 2] = total.astype(bf16)
        if i == last:
            yback[i, h] = fsend[2 * i + h]
            src = fsend.at[2 * i + 1 - h]
            begin(remote(src, yback.at[i, h], fy_s.at[0], fy_r.at[i, h], mate))
            return
        if i == far:
            half[...] = total
            copy = remote(fsend.at[2 * i + 1 - h], qrecv, qy_s.at[0], qy_r.at[0], mate)
            pending["i", i] = begin(copy)
            return
        for side in (0, 1):
            way = hops[i] + 1 if side else ys_n - hops[i]
            back = at(z, lax.rem(2 * pair + way, ys_n), c, x)
            k = 2 * i + side
            begin(remote(fsend.at[k], yback.at[i, h], fy_s.at[0], fy_r.at[i, h], back))

    def step_j(i):
        with jax.named_scope(f"j_wait{i}"):
            pending["i", i].wait_recv()
        fsend[2 * i + h] = (half[h] + qrecv[...].astype(f32)).astype(bf16)
        back = at(z, lax.rem(y + ys_n + hops[i] * (2 * h - 1), ys_n), c, x)
        k = 2 * i + h
        begin(remote(fsend.at[k], yback.at[i, 0], fy_s.at[0], fy_r.at[i, 0], back))

    def back_wait(i, hh):
        ref = yback.at[i, hh]
        remote(ref, ref, fy_s.at[0], fy_r.at[i, hh], mate).wait_recv()

    def zb_all(n):
        base = sum(g_rows[:n])
        ref = zgot.at[pl.ds(0, zs_n - 1), pl.ds(base, g_rows[n])]
        return remote(ref, ref, zb_s.at[n], zb_r.at[n], partner)

    def z_return(n):
        group, step = groups[n], g_rows[n]
        many = len(group) * erow
        perms = [
            unpermutation(many, zs_n * step, step, 1.0 * cc * len(group) * cap)
            for cc in range(parts)
        ]
        with jax.named_scope(f"back_wait{n}"):
            for i in group:
                if i == last:
                    back_wait(i, 1 - h)
                elif i == far:
                    back_wait(i, 0)
                else:
                    back_wait(i, 0)
                    back_wait(i, 1)
        moved = 0.0
        for hh in (0,) if group == [far] else (0, 1):
            rows = yback[group[0] : group[-1] + 1, hh].reshape(many, dx)
            for cc, perm in enumerate(perms):
                piece = rows[:, cc * lanes : (cc + 1) * lanes]
                moved = moved + jnp.dot(perm, piece, preferred_element_type=f32)
        base = sum(g_rows[:n])
        zback[:, base : base + step] = moved.astype(bf16).reshape(zs_n, step, lanes)
        rows = pl.ds(base, step)
        kept = []
        for r in near:
            zt = zpeer(r)
            copy = remote(
                zback.at[zt, rows], zgot.at[z, rows], zb_s.at[n], zb_r.at[n], at(zt, y, c, x)
            )
            copy.start()
            kept.append(copy)
        zgot[z, base : base + step] = zback[z, base : base + step]
        backs_z.extend(kept)
        returned.append((n, kept))

    def branch_core():
        with jax.named_scope("bz_wait"):
            bz_all().wait_recv()
        begin(remote(bw.at[:, :, :, c], bw.at[:, :, :, c], bc_s.at[0], bc_r.at[0], partner))

    def branch_dense():
        ref = bw.at[:, :, :, 1 - c]
        remote(ref, ref, bc_s.at[0], bc_r.at[0], partner).wait_recv()
        whole_in = bw[0].reshape(width, bw.shape[5])
        pre = jnp.dot(normed[...], whole_in, preferred_element_type=f32)
        hb = (pre / (1.0 + jnp.exp(-pre))).astype(bf16)
        for xx in range(xs_n):
            zpart = zs_n // xs_n if zs_n >= xs_n else 0
            if zpart:
                wo = bw[1, xx * zpart : (xx + 1) * zpart].reshape(dx, bw.shape[5])
            else:
                wo = bw[1].reshape(width, bw.shape[5])[xx * dx : (xx + 1) * dx]
            term = lax.dot_general(hb, wo, (((1,), (1,)), ((), ())), preferred_element_type=f32)
            bterm[xx] = term.astype(bf16)

    def branch_send():
        for r in range(1, xs_n):
            xt = xpeer(r)
            copy = remote(bterm.at[xt], bgot.at[r], bx_s.at[0], bx_r.at[0], at(z, y, c, xt))
            copy.start()
            bx.append(copy)

    order = ("d0", "d1", "n0", "m0", "d2", "n1", "b0", "m1", "n2", "c0", "b1", "o1", "m2", "planes", "e0", "b2", "c1", "e1", "c2", "e2", "f1", "f0", "o2", "e3", "f2", "g1", "i1", "g2", "g0", "core", "i2", "i0", "f3", "dense", "j2", "g3", "z0", "i3", "send", "z2", "z1")
    steps = dict(b=step_b, c=step_c, d=step_d, e=step_e, f=step_f, g=step_g, i=step_i, j=step_j)
    steps.update(m=step_m, n=step_n, o=step_o, z=z_return)
    others = dict(planes=branch_planes, core=branch_core, dense=branch_dense, send=branch_send)
    for item in order:
        if item in others:
            others[item]()
        else:
            steps[item[0]](int(item[1]))

    diff = scores_t[0:1, :] - scores_t[1:2, :]
    mixes = []
    for d in (diff, -diff):
        row = jnp.broadcast_to(sigmoid(d), sq)
        mixes.append(jnp.sum(jnp.where(sq_a == sq_b, row, 0.0), axis=1, keepdims=True))

    def column(row):
        wide_row = jnp.broadcast_to(row, sq)
        return jnp.sum(jnp.where(sq_a == sq_b, wide_row, 0.0), axis=1, keepdims=True)

    spots = [column(come[r]) for r in (0, 1)]

    def picks(n):
        shape = (rows_tok, zs_n * g_rows[n])
        t = lax.broadcasted_iota(jnp.int32, shape, 1).astype(f32) + 1.0 * g_low[n]
        size = len(groups[n]) * cap
        return [
            [jnp.where(t == spots[r] + 1.0 * cc * size, 1.0, 0.0).astype(bf16) for cc in range(parts)]
            for r in (0, 1)
        ]

    def combine(n, taken):
        base = sum(g_rows[:n])
        rows = zgot[:, base : base + g_rows[n]].reshape(zs_n * g_rows[n], lanes)
        terms = []
        for cc in range(parts):
            one = jnp.dot(taken[0][cc], rows, preferred_element_type=f32)
            two = jnp.dot(taken[1][cc], rows, preferred_element_type=f32)
            terms.append(mixes[0] * one + mixes[1] * two)
        return jnp.concatenate(terms, axis=1)

    with jax.named_scope("bx_wait"):
        bx_all().wait_recv()
    share = bterm[x].astype(f32)
    for r in range(1, xs_n):
        share = share + bgot[r].astype(f32)
    share = share * branch_weight
    for n, _ in returned:
        taken = picks(n)
        with jax.named_scope(f"kept{n}"):
            if near:
                zb_all(n).wait_recv()
        share = share + combine(n, taken)
    out[...] = share.astype(out.dtype)

    with jax.named_scope("send_wait"):
        if near:
            for i in range(1, pairs):
                zd_all(i).wait_send()
            for n in range(len(groups)):
                zb_all(n).wait_send()
            by_all().wait_send()
        bz_all().wait_send()
        bx_all().wait_send()
        narrow = 2 * last
        for ref, sem in (
            (tok.at[pl.ds(0, last), :, :, pl.ds(0, 3 * dx)], tx_s),
            (hid.at[:, :, :, pl.ds(0, 3 * fx)], hx_s),
            (tok.at[:, 0], tc_s),
            (tok.at[pl.ds(0, last + 2), :, :, pl.ds(0, dx)], yd_s),
            (fsend.at[pl.ds(0, narrow)], fy_s),
            (psend.at[:, 0], pc_s),
            (qrecv, qy_s),
            (bw.at[:, :, :, 0], bc_s),
        ):
            remote(ref, ref, sem.at[0], qy_r.at[0], partner).wait_send()


def on_device(
    cores_z,
    cores_y,
    tokens,
    norm_gain,
    routes,
    route_scores,
    expert_gate,
    expert_up,
    expert_down,
    branch_in,
    branch_out,
    branch_gate,
):
    zs_n, ys_n = cores_z, cores_y
    xs_n = lax.axis_size("tp")
    rows_tok, width = tokens.shape
    experts = zs_n * ys_n // 2
    cap = 5 * rows_tok * routes.shape[1] // (4 * experts)
    pairs = ys_n // 2
    dx = width // xs_n
    fx = expert_gate.shape[2]
    fg = expert_down.shape[1]
    arow = round_up(dx // 128 * cap, 16)
    erow = round_up(zs_n * cap, 16)
    back_rows = sum(round_up(dx // 128 * len(g) * cap, 16) for g in return_groups(pairs))
    bpart = branch_in.shape
    bf16, f32 = jnp.bfloat16, jnp.float32
    vm = lambda shape, dtype=bf16: pltpu.VMEM(shape, dtype)
    sem = lambda *shape: pltpu.SemaphoreType.DMA(shape)
    scratch = [
        vm((rows_tok, width)),
        vm((1, width), f32),
        vm((2, rows_tok), jnp.int32),
        vm((2, rows_tok), f32),
        vm((1, width), f32),
        vm(bpart),
        vm(bpart),
        vm((rows_tok, width)),
        vm((pairs - 1, zs_n, arow, 128)),
        vm((pairs - 1, zs_n, arow, 128)),
        vm((zs_n, arow, width // (dx // 128))),
        vm((zs_n, arow, width // (dx // 128))),
        vm((pairs - 1, erow, dx)),
        vm((ys_n, CORES, erow, width)),
        vm((width, 2 * fx)),
        vm((fg, dx)),
        vm((ys_n, CORES, erow, fg)),
        vm((pairs, 2, CORES, erow, dx), f32),
        vm((ys_n, CORES, erow, dx)),
        vm((ys_n, erow, dx)),
        vm((dx // 128, erow, zs_n * arow)),
        vm((2, erow, dx), f32),
        vm((erow, dx)),
        vm((ys_n, erow, dx)),
        vm((pairs, 2, erow, dx)),
        vm((zs_n, back_rows, 128)),
        vm((zs_n, back_rows, 128)),
        vm((2, zs_n, ys_n, CORES, *bpart)),
        vm((xs_n, rows_tok, dx)),
        vm((xs_n, rows_tok, dx)),
        sem(10),
        sem(pairs),
        sem(pairs),
        sem(1),
        sem(ys_n),
        sem(1),
        sem(3, ys_n),
        sem(1),
        sem(ys_n),
        sem(1),
        sem(3, ys_n),
        sem(1),
        sem(pairs),
        sem(1),
        sem(1),
        sem(1),
        sem(pairs, 2),
        sem(pairs),
        sem(pairs),
        sem(1),
        sem(1),
        sem(1),
        sem(1),
        sem(1),
        sem(1),
        sem(1),
        sem(1),
    ]
    in_vmem = pl.BlockSpec(memory_space=pltpu.VMEM)
    in_hbm = pl.BlockSpec(memory_space=pl.ANY)
    return pl.pallas_call(
        functools.partial(layer_kernel, zs_n, ys_n, xs_n, cap),
        out_shape=jax.ShapeDtypeStruct((rows_tok, dx), bf16),
        in_specs=[in_hbm] * 10,
        out_specs=in_vmem,
        scratch_shapes=scratch,
        compiler_params=pltpu.CompilerParams(
            collective_id=0, has_side_effects=True, vmem_limit_bytes=60 * 1024 * 1024
        ),
        name="routed_layer",
    )(
        tokens,
        norm_gain.reshape(1, -1),
        routes.T,
        route_scores.T,
        branch_gate.reshape(1, -1),
        branch_in,
        branch_out.T,
        expert_gate,
        expert_up,
        expert_down,
    )


def solution(mesh, z_y=None):
    ep = mesh.shape["ep"]
    zs_n, ys_n = z_y or (8, ep // (8 * CORES))
    in_specs = (
        P("ep", None),
        P(),
        P("ep", None),
        P("ep", None),
        P("ep", None, "tp"),
        P("ep", None, "tp"),
        P("ep", None, "tp"),
        P("ep", "tp"),
        P("tp", "ep"),
        P(),
    )
    return jax.shard_map(
        functools.partial(on_device, zs_n, ys_n),
        mesh=mesh,
        in_specs=in_specs,
        out_specs=P("ep", "tp"),
        check_vma=False,
    )
```
